32 devices in a mesh: sp: 4 (over y, x), tp: 8 (over z, core).
Axes of the slice: x: 2, y: 2, z: 4, core: 2. Of those that a mesh axis runs over, the one named last changes fastest.
Arguments:
- stream: bfloat16 [4096, 1024], P('tp', 'sp'), may hold values from -6 to 6
- value_weight: bfloat16 [2, 2048, 4096], P(None, 'tp', 'sp'), may hold values from -0.09375 to 0.09375
- gate_weight: bfloat16 [2, 2048, 4096], P(None, 'tp', 'sp'), may hold values from -0.09375 to 0.09375
- conv_taps: bfloat16 [2, 2048, 31], P(None, 'tp'), may hold values from -16 to 16
- norm_gain: bfloat16 [2, 2048], P(None, 'tp'), may hold values from 0.099609375 to 1.8984375
- out_weight: bfloat16 [2, 4096, 2048], P(None, 'tp', 'sp'), may hold values from -4 to 4
- out_gain: bfloat16 [2, 4096], P(None, 'tp'), may hold values from 0.099609375 to 1.8984375
Outputs:
- result: bfloat16 [4096, 1024], P('tp', 'sp')
The draws below stay inside these ranges and needn't reach their ends.
All inputs are finite; a program needn't handle non-finite values.
Results may differ from the reference program's by a relative error of at most 0.015.
Values may be sent and summed in bfloat16 or wider, within the bound.
A program may use at most 64 MiB of HBM per device.

```python
import jax
import jax.numpy as jnp
from jax import lax

D = 4096
W = 2048
KERNEL = 31
LAYERS = 2
SEQ = 1024


def rising_draw(key, shape, fan, axis):
    base = jax.random.normal(key, shape, jnp.float32)
    position = lax.broadcasted_iota(jnp.float32, shape, axis) / shape[axis]
    return base * fan ** (-0.5) * jnp.exp(position * 2.302585)


def draw_conv_taps(key, part):
    return rising_draw(jax.random.fold_in(key, 11), (LAYERS, W, KERNEL), KERNEL, 1).astype(jnp.bfloat16)


def draw_out_weight(key, part):
    return rising_draw(jax.random.fold_in(key, 23), (LAYERS, D, W), W, 1).astype(jnp.bfloat16)


def levels(key, shape, cuts, least, largest):
    loudness, own = 1.0, jax.random.fold_in(key, 6)
    for dim, blocks in cuts:
        steps = jnp.exp(jax.random.uniform(jax.random.fold_in(own, dim), (blocks,), jnp.float32, least / len(cuts), largest / len(cuts)))
        loudness = loudness * jnp.repeat(steps, shape[dim] // blocks).reshape([-1 if axis == dim else 1 for axis in range(len(shape))])
    return loudness


def gaussian(own_key, extent, scale, bound, pieces=(), dtype=jnp.bfloat16):
    gain = levels(own_key, extent, pieces, -0.22, 0.18) if pieces else 1.0
    result = jax.random.normal(own_key, extent, jnp.float32) * scale * gain
    return jnp.minimum(jnp.maximum(result, -bound), bound).astype(dtype)


def setup_inputs(seed: int = 0) -> dict:
    splits = jax.random.split(jax.random.key(seed), 8)
    stream = gaussian(splits[0], (D, SEQ), 1.0, 6.0, ((0, 8), (1, 4)))
    value_weight = gaussian(splits[1], (LAYERS, W, D), D ** -0.5, 0.09375, ((1, 8), (2, 4)))
    gate_weight = gaussian(splits[2], (LAYERS, W, D), D ** -0.5, 0.09375, ((1, 8), (2, 4)))
    conv_taps = draw_conv_taps(jax.random.fold_in(splits[7], 71), 0)
    norm_gain = jnp.clip(1.0 + 0.18 * jax.random.normal(splits[4], (LAYERS, W), jnp.float32), 0.099609375, 1.8984375).astype(jnp.bfloat16)
    out_weight = draw_out_weight(jax.random.fold_in(splits[7], 71), 0)
    out_gain = jnp.clip(1.0 + 0.18 * jax.random.normal(splits[6], (LAYERS, D), jnp.float32), 0.099609375, 1.8984375).astype(jnp.bfloat16)
    return {"stream": stream, "value_weight": value_weight, "gate_weight": gate_weight, "conv_taps": conv_taps, "norm_gain": norm_gain, "out_weight": out_weight, "out_gain": out_gain}


def reference(stream, value_weight, gate_weight, conv_taps, norm_gain, out_weight, out_gain):
    hidden = stream
    reach = KERNEL // 2
    for layer_index in range(LAYERS):
        value_proj = jnp.dot(value_weight[layer_index], hidden, preferred_element_type=jnp.float32)
        gate_proj = jnp.dot(gate_weight[layer_index], hidden, preferred_element_type=jnp.float32)
        gated = (value_proj * jax.nn.sigmoid(gate_proj)).astype(jnp.bfloat16)
        padded = jnp.pad(gated.astype(jnp.float32), ((0, 0), (reach, reach)))
        kernel_taps = conv_taps[layer_index].astype(jnp.float32)
        convolved = jnp.zeros((W, SEQ), jnp.float32)
        for offset in range(KERNEL):
            convolved = convolved + kernel_taps[:, offset:offset + 1] * padded[:, offset:offset + SEQ]
        conv_wide = lax.optimization_barrier(convolved.astype(jnp.bfloat16)).astype(jnp.float32)
        average = lax.optimization_barrier(jnp.sum(conv_wide, axis=0)) / W
        variance = lax.optimization_barrier(jnp.sum(conv_wide * conv_wide, axis=0)) / W - average * average
        channel_gain = norm_gain[layer_index].astype(jnp.float32)[:, None]
        activated = jax.nn.silu((conv_wide - average) * lax.rsqrt(variance + 1e-05) * channel_gain).astype(jnp.bfloat16)
        branch = jnp.dot(out_weight[layer_index], activated, preferred_element_type=jnp.float32)
        branch_wide = lax.optimization_barrier(branch.astype(jnp.bfloat16)).astype(jnp.float32)
        square_mean = lax.optimization_barrier(jnp.sum(branch_wide * branch_wide, axis=0)) / D
        feature_gain = out_gain[layer_index].astype(jnp.float32)[:, None]
        hidden = (hidden.astype(jnp.float32) + branch_wide * lax.rsqrt(square_mean + 1e-06) * feature_gain).astype(jnp.bfloat16)
    return hidden
```

```python
import functools

import jax
import jax.numpy as jnp
from jax import lax
from jax.experimental import pallas as pl
from jax.experimental.pallas import tpu as pltpu
from jax.sharding import PartitionSpec as P

MESH = pl.DeviceIdType.MESH
F32 = jnp.float32
BF16 = jnp.bfloat16
LANES = 128
EDGE = 16
TILE = 64


def grid_of(count):
    nx = int(count**0.5)
    while count % nx:
        nx -= 1
    return count // nx, nx


def pieces_of(rows, size):
    return max(1, rows // size)


def kernel(
    n_sp, n_tp, n_layers,
    stream, value_w, gate_w, taps, norm_gain, out_w, out_gain,
    result,
    h_all, x_all, conv_all, branch_all, active, v_buf, g_buf, o_buf, part_out, part_in, wide, flat, tap_rows,
    acc, sums, squares, norm_rows, out_rows, norm_cols, out_cols,
    local_sem, send_sem, recv_sem,
):
    ny, nx = grid_of(n_sp)
    nz = n_tp // 2
    s, t = lax.axis_index("sp"), lax.axis_index("tp")
    y, x = s // nx, s % nx
    z, c = t // 2, t % 2
    features, positions = stream.shape
    channels = value_w.shape[1]
    f_cols = value_w.shape[2]
    c_cols = out_w.shape[2]
    width = channels * n_tp
    model = features * n_tp
    n_taps = taps.shape[2]
    reach = n_taps // 2
    groups = pieces_of(channels, LANES)
    group = channels // groups
    counter = [0]
    sent = []

    def remote(src, dst, sp, tp, width=1, pick=0):
        i = counter[0]
        counter[0] += width
        return pltpu.make_async_remote_copy(
            src_ref=src, dst_ref=dst, send_sem=send_sem.at[i], recv_sem=recv_sem.at[i + pick],
            device_id={"sp": sp, "tp": tp}, device_id_type=MESH,
        )

    def start(copy, condition=None):
        if condition is None:
            copy.start()
        else:
            pl.when(condition)(copy.start)
        sent.append((copy, condition))

    def slot_of(k, j):
        return lax.rem(y + ny - k, ny) * nx + lax.rem(x + nx - j, nx)

    def x_peer(j):
        return y * nx + lax.rem(x + j, nx)

    def y_peer(k):
        return lax.rem(y + k, ny) * nx + x

    local_count = [0]

    def local_copy(src, dst):
        i = local_count[0]
        local_count[0] += 1
        copy = pltpu.make_async_copy(src, dst, local_sem.at[i])
        copy.start()
        return copy

    class Gather:
        def __init__(self, src, dst, x_first, whole=True):
            self.copies, self.own_x, self.own_y, self.relays = {}, [], [], []
            for k in range(ny):
                for j in range(nx if whole else 1):
                    if k == 0 and j == 0:
                        continue
                    if x_first:
                        along_x = k == 0
                        origin = (0, 0) if along_x else (0, j)
                    else:
                        along_x = j > 0
                        origin = (k, 0) if along_x else (0, 0)
                    own = origin == (0, 0)
                    target = x_peer(j) if along_x else y_peer(k)
                    origin_slot = slot_of(*origin)
                    copy = remote(src if own else dst(origin_slot), dst(origin_slot), target, t)
                    self.copies[k, j] = copy
                    if not own:
                        self.relays.append((copy, origin))
                    elif along_x:
                        self.own_x.append(copy)
                    else:
                        self.own_y.append(copy)
            self.local = local_copy(src, dst(s))
            self.here, self.done = set(), set()

        def once(self, name):
            fresh = name not in self.done
            self.done.add(name)
            return fresh

        def send_x(self):
            if self.once("x"):
                for copy in self.own_x:
                    start(copy)

        def send_y(self):
            if self.once("y"):
                for copy in self.own_y:
                    start(copy)

        def relay(self):
            if self.once("relay"):
                for copy, origin in self.relays:
                    self.arrive(*origin)
                    start(copy)

        def flush(self):
            self.send_x()
            self.send_y()
            self.relay()

        def arrive(self, k, j):
            if (k, j) not in self.here:
                self.here.add((k, j))
                if k == 0 and j == 0:
                    self.local.wait()
                else:
                    self.copies[k, j].wait_recv()

    def gathers(w_ref, buf, l, orders, whole=True):
        rows = w_ref.shape[1] // len(orders)
        made = []
        for i, x_first in enumerate(orders):
            part = pl.ds(i * rows, rows)
            made.append(Gather(w_ref.at[l, part], lambda q, part=part: buf.at[l, q, part], x_first, whole))
        return made

    class Spread:
        def __init__(self, buf, rows, pieces, src):
            size = rows // pieces

            def place(zz, cc, k):
                row = pl.multiple_of((jnp.clip(zz, 0, nz - 1) * 2 + cc) * rows + k * size, size)
                return buf.at[pl.ds(row, size), :]

            self.pieces, self.place, self.src = pieces, place, src
            self.across = [remote(src(k), place(z, c, k), s, z * 2 + 1 - c) for k in range(pieces)]
            self.along, self.hand, self.has = {}, {}, {}
            for way in (1, -1):
                after = jnp.clip(z + way, 0, nz - 1) * 2 + c
                for d in range(1, nz):
                    self.has[way, d] = (z - way * d >= 0) & (z - way * d < nz)
                    for k in range(pieces):
                        carried = z - way * (d - 1)
                        origin = src(k) if d == 1 else place(carried, c, k)
                        self.along[way, d, k] = remote(origin, place(carried, c, k), s, after)
                        seen = place(z - way * d, c, k)
                        self.hand[way, d, k] = remote(seen, seen, s, z * 2 + 1 - c)

        def send(self, way, d, k):
            holds = (z - way * (d - 1) >= 0) & (z - way * (d - 1) < nz)
            more = (z + way >= 0) & (z + way < nz)
            start(self.along[way, d, k], holds & more)

        def start_own(self, k):
            for way in (1, -1):
                self.send(way, 1, k)
            start(self.across[k])

        def step(self, d, k, extra=None):
            for way in (1, -1):
                pl.when(self.has[way, d])(self.along[way, d, k].wait_recv)
                if d + 1 < nz:
                    self.send(way, d + 1, k)
                start(self.hand[way, d, k], self.has[way, d])
                if extra is not None:
                    extra(way, d, k)

        def wait_across(self):
            for copy in self.across:
                copy.wait_recv()

        def wait_hand(self, way, d):
            for k in range(self.pieces):
                self.hand[way, d, k].wait_recv()

    class Cross:
        def __init__(self, spread):
            self.spread = spread
            self.size = features // spread.pieces
            self.base, self.hands = {}, {}

        def facts(self, way, d):
            zz = z - way * d
            ok = (zz >= 0) & (zz < nz)
            q = jnp.clip(zz, 0, nz - 1)
            return ok, q, lax.rem(q, nx)

        def rows(self, q, k):
            row = (q // nx * 2 + c) * features + k * self.size
            return pl.ds(pl.multiple_of(row, self.size), self.size)

        def forward(self, way, d, k):
            ok, q, owner = self.facts(way, d)
            pick = jnp.clip(lax.rem(owner - x + nx, nx) - 1, 0, nx - 2)
            self.base[way, d, k] = counter[0]
            src = self.spread.src(k) if d == 0 else self.spread.place(q, c, k)
            copy = remote(
                src, x_all.at[pick, self.rows(q, k), :], y * nx + owner, t, width=nx - 1, pick=pick
            )
            start(copy, ok & (owner != x))

        def receive(self, way, d, k):
            ok, q, owner = self.facts(way, d)
            mine = ok & (owner == x)
            base = self.base[way, d, k]
            for j in range(1, nx):
                here = x_all.at[j - 1, self.rows(q, k), :]
                landed = pltpu.make_async_remote_copy(
                    src_ref=here, dst_ref=here, send_sem=send_sem.at[base], recv_sem=recv_sem.at[base + j - 1],
                    device_id={"sp": s, "tp": z * 2 + 1 - c}, device_id_type=MESH,
                )
                pl.when(mine)(landed.wait_recv)
                hand = remote(here, here, s, z * 2 + 1 - c)
                start(hand, mine)
                self.hands[way, d, k, j] = (hand, mine)

        def finish(self):
            for hand, mine in self.hands.values():
                pl.when(mine)(hand.wait_recv)

    def exchange(src, buf):
        copies = []
        for k in range(1, n_tp):
            copies.append(remote(src, buf.at[t], s, lax.rem(t + k, n_tp)))
            start(copies[-1])
        return copies

    def arrived(copies):
        for copy in copies:
            copy.wait_recv()

    my_rows = pl.ds(pl.multiple_of(t * features, features), features)
    my_channels = pl.ds(pl.multiple_of(t * channels, channels), channels)
    stream_pieces = pieces_of(features, 128)
    conv_pieces = groups * pieces_of(group, 64)

    def rows_of(ref, rows, pieces):
        size = rows // pieces
        return lambda k: ref.at[pl.ds(k * size, size), :]

    stream_copy = local_copy(stream, h_all.at[0, my_rows, :])
    barrier = pltpu.get_barrier_semaphore()
    for k in range(1, n_sp):
        pl.semaphore_signal(
            barrier, inc=1, device_id={"sp": lax.rem(s + k, n_sp), "tp": t}, device_id_type=MESH
        )
    for k in range(1, n_tp):
        pl.semaphore_signal(
            barrier, inc=1, device_id={"sp": s, "tp": lax.rem(t + k, n_tp)}, device_id_type=MESH
        )
    in_proj, out_proj = [], []
    out_parts = pieces_of(features, 128)
    for l in range(n_layers):
        if l == 0:
            v_parts = gathers(value_w, v_buf, l, [True], whole=False)
            g_parts = gathers(gate_w, g_buf, l, [True], whole=False)
        else:
            v_parts = gathers(value_w, v_buf, l, [True, True])
            g_parts = gathers(gate_w, g_buf, l, [False, False])
        in_proj.append((v_parts, g_parts))
        last = l + 1 == n_layers
        out_proj.append(gathers(out_w, o_buf, l, [last] * out_parts))
    norm_rows[t] = norm_gain[...]
    out_rows[t] = out_gain[...]
    for l in range(n_layers):
        padded = jnp.concatenate([taps[l].astype(F32), jnp.zeros((channels, LANES - n_taps), F32)], axis=1)
        tap_rows[l] = padded.T[: 2 * EDGE]
    stream_copy.wait()
    pl.semaphore_wait(barrier, n_sp + n_tp - 2)

    spread = Spread(
        h_all.at[0], features, stream_pieces, rows_of(h_all.at[0, my_rows, :], features, stream_pieces)
    )
    cross = Cross(spread)
    for k in range(stream_pieces):
        spread.start_own(k)
        cross.forward(1, 0, k)
    for part in in_proj[0][0] + in_proj[0][1]:
        part.send_y()
    out_proj[0][0].send_x()
    gain_copies = exchange(norm_gain, norm_rows) + exchange(out_gain, out_rows)

    def to_columns(rows_ref, cols_ref, count):
        def turn(i, carry):
            rows = rows_ref[i].astype(F32)
            fill = jnp.zeros((8 - n_layers, count), F32)
            place = pl.ds(pl.multiple_of(i * count, count), count)
            cols_ref[place, :] = jnp.concatenate([rows, fill], axis=0).T
            return carry

        lax.fori_loop(0, n_tp, turn, 0)

    steps = [(k, j) for k in range(ny) for j in range(nx)]
    right, left = lax.rem(s + 1, n_sp), lax.rem(s + n_sp - 1, n_sp)
    has_right, has_left = s < n_sp - 1, s > 0

    def rows_at(q, count):
        return pl.ds(pl.multiple_of(q * count, count), count)

    for l in range(n_layers):
        last = l + 1 == n_layers
        following = None if last else in_proj[l + 1]
        groups_of_rows = [pl.ds(m * group, group) for m in range(groups)]
        if l == 0:
            waiting = list(out_proj[0][1:])
            for d in range(1, nz):
                if d == nz - 1:
                    arrived(gain_copies)
                    to_columns(norm_rows, norm_cols, channels)
                    to_columns(out_rows, out_cols, features)
                for k in range(stream_pieces):
                    spread.step(d, k, cross.forward)
                    for way in ((1,) if d == 1 else (1, -1)):
                        cross.receive(way, d - 1, k)
                    if waiting and ((d - 1) * stream_pieces + k) % 2 == 1:
                        waiting.pop(0).send_x()
            for part in waiting:
                part.send_x()
            spread.wait_across()
            for d in range(1, nz):
                for way in (1, -1):
                    @pl.when(spread.has[way, d])
                    def _():
                        spread.wait_hand(way, d)
            for half, (parts, buf) in enumerate(zip(in_proj[l], (v_buf, g_buf))):
                total = None
                for k in range(ny):
                    for part in parts:
                        part.arrive(k, 0)
                    slot = slot_of(k, 0)
                    one = jnp.dot(buf[l, slot], h_all[l, rows_at(slot, f_cols), :], preferred_element_type=F32)
                    total = one if total is None else total + one
                acc[half] = total
            for k in range(stream_pieces):
                for way in (1, -1):
                    cross.receive(way, nz - 1, k)
            cross.finish()
            part_copies = {}
            for m, rows in enumerate(groups_of_rows):
                for j in range(1, nx):
                    for half, buf in enumerate((v_buf, g_buf)):
                        total = None
                        for k in range(ny):
                            block = rows_at(lax.rem(y + ny - k, ny), f_cols)
                            one = jnp.dot(
                                buf[l, slot_of(k, 0), rows, :], x_all[j - 1, block, :],
                                preferred_element_type=F32,
                            )
                            total = one if total is None else total + one
                        part_out[j - 1, half, rows, :] = total.astype(BF16)
                    copy = remote(
                        part_out.at[j - 1, :, rows, :], part_in.at[j - 1, :, rows, :],
                        y * nx + lax.rem(x + nx - j, nx), t,
                    )
                    start(copy)
                    part_copies[m, j] = copy
            for part in out_proj[0]:
                part.send_y()
        else:
            for part in in_proj[l][0] + in_proj[l][1]:
                part.flush()
            for k, j in steps:
                slot = slot_of(k, j)
                for half, (parts, buf) in enumerate(zip(in_proj[l], (v_buf, g_buf))):
                    for part in parts:
                        part.arrive(k, j)
                    one = jnp.dot(buf[l, slot], h_all[l, rows_at(slot, f_cols), :], preferred_element_type=F32)
                    if (k, j) == (0, 0):
                        acc[half] = one
                    else:
                        acc[half] += one

        edges = []
        for m, rows in enumerate(groups_of_rows):
            lanes = pl.ds(m * group, group)
            value, gate = acc[0, rows, :], acc[1, rows, :]
            if l == 0:
                for j in range(1, nx):
                    part_copies[m, j].wait_recv()
                    value = value + part_in[j - 1, 0, rows, :].astype(F32)
                    gate = gate + part_in[j - 1, 1, rows, :].astype(F32)
            gated = (value * jax.nn.sigmoid(gate)).astype(BF16)
            wide[l, pl.ds(EDGE, positions), lanes] = gated.astype(F32).T
            to_right = remote(
                wide.at[l, pl.ds(positions, EDGE), lanes], wide.at[l, pl.ds(0, EDGE), lanes], right, t
            )
            to_left = remote(
                wide.at[l, pl.ds(EDGE, EDGE), lanes], wide.at[l, pl.ds(EDGE + positions, EDGE), lanes], left, t
            )
            start(to_right, has_right)
            start(to_left, has_left)
            edges.append((to_right, to_left))

        if l == 0:
            if following is not None:
                following[0][0].send_x()
                for part in following[1] + following[0]:
                    part.send_y()
        if last:
            for part in out_proj[l]:
                part.send_x()

        blank = jnp.zeros((EDGE, channels), F32)

        @pl.when(s == 0)
        def _():
            wide[l, 0:EDGE, :] = blank

        @pl.when(s == n_sp - 1)
        def _():
            wide[l, EDGE + positions : 2 * EDGE + positions, :] = blank

        conv_size = channels // conv_pieces
        conv_spread = Spread(
            conv_all.at[l], channels, conv_pieces, rows_of(conv_all.at[l, my_channels, :], channels, conv_pieces)
        )
        own_sum = own_square = None
        for m in range(groups):
            lanes = pl.ds(m * group, group)
            to_right, to_left = edges[m]
            pl.when(has_left)(to_right.wait_recv)
            pl.when(has_right)(to_left.wait_recv)
            def conv_step(i, carry, lanes=lanes):
                first = pl.multiple_of(i * TILE, TILE)
                extent = TILE + 2 * EDGE
                window = wide[l, pl.ds(first, extent), lanes]
                total = None
                for r in range(8):
                    moved = window if r == 0 else pltpu.roll(window, extent - r, 0)
                    for q in range(0, 2 * EDGE + 1, 8):
                        tap = q + r - (EDGE - reach)
                        if 0 <= tap < n_taps:
                            term = tap_rows[l, tap : tap + 1, lanes] * moved[q : q + TILE]
                            total = term if total is None else total + term
                flat[pl.ds(first, TILE), lanes] = total
                return carry

            lax.fori_loop(0, positions // TILE, conv_step, 0)
            narrow = flat[:, lanes].T.astype(BF16)
            row = pl.multiple_of(t * channels + m * group, group)
            conv_all[l, pl.ds(row, group), :] = narrow
            for k in range(m * (group // conv_size), (m + 1) * (group // conv_size)):
                conv_spread.start_own(k)
            seen = narrow.astype(F32)
            part_sum = jnp.sum(seen, axis=0, keepdims=True)
            part_square = jnp.sum(seen * seen, axis=0, keepdims=True)
            own_sum = part_sum if own_sum is None else own_sum + part_sum
            own_square = part_square if own_square is None else own_square + part_square
        sums[l, t, 0:1, :] = own_sum
        sums[l, t, 1:2, :] = own_square
        sum_copies = exchange(sums.at[l, t], sums.at[l])

        turn = [None]

        def settle():
            arrived(sum_copies)
            totals = jnp.sum(sums[l], axis=0)
            average = totals[0:1] / width
            variance = totals[1:2] / width - average * average
            turn[0] = (average, lax.rsqrt(variance + 1e-05))

        def activate(block):
            average, inverse = turn[0]
            rows = rows_at(block, channels)
            gain = norm_cols[rows, l : l + 1]
            scaled = (conv_all[l, rows, :].astype(F32) - average) * inverse * gain
            active[rows, :] = (scaled / (1.0 + jnp.exp(-scaled))).astype(BF16)

        def drain(spread, ready, consume, hook):
            def take(d):
                for way in (1, -1):
                    @pl.when(spread.has[way, d])
                    def _():
                        consume((z - way * d) * 2 + c)
                        spread.wait_hand(way, d)
                        consume((z - way * d) * 2 + 1 - c)

            when = min(2, nz - 1)
            for d in range(1, nz):
                for k in range(spread.pieces):
                    spread.step(d, k)
                    hook((d - 1) * spread.pieces + k)
                if d == when:
                    ready()
                    consume(t)
                    spread.wait_across()
                    consume(z * 2 + 1 - c)
                if d >= when and d > 1:
                    take(d - 1)
            take(nz - 1)

        def conv_hook(i):
            if l == 0:
                if i == 1:
                    for part in out_proj[l][: out_parts // 2]:
                        part.relay()
                if i == 4:
                    for part in out_proj[l][out_parts // 2 :]:
                        part.relay()
                if i == 5 and following is not None:
                    following[0][1].send_x()
            if last and i % 3 == 0 and 0 < i // 3 <= out_parts:
                out_proj[l][i // 3 - 1].flush()

        drain(conv_spread, settle, activate, conv_hook)
        for part in out_proj[l]:
            part.flush()
        total = None
        for k, j in steps:
            slot = slot_of(k, j)
            for part in out_proj[l]:
                part.arrive(k, j)
            one = jnp.dot(o_buf[l, slot], active[rows_at(slot, c_cols), :], preferred_element_type=F32)
            total = one if total is None else total + one
        narrow_branch = total.astype(BF16)
        branch = narrow_branch.astype(F32)
        squares[l, t, 0:1, :] = jnp.sum(branch * branch, axis=0, keepdims=True)
        square_copies = exchange(squares.at[l, t], squares.at[l])

        def factor_of():
            arrived(square_copies)
            return lax.rsqrt(jnp.sum(squares[l], axis=0) / model + 1e-06)

        if last:
            factor = factor_of()
            gain = out_cols[my_rows, l : l + 1]
            fresh = h_all[l, my_rows, :].astype(F32) + branch * factor * gain
            result[...] = fresh.astype(BF16)
        else:
            branch_all[l, my_rows, :] = narrow_branch
            branch_spread = Spread(
                branch_all.at[l], features, stream_pieces,
                rows_of(branch_all.at[l, my_rows, :], features, stream_pieces),
            )
            for k in range(stream_pieces):
                branch_spread.start_own(k)
            if l == 0:
                for part in following[0] + following[1]:
                    part.send_x()

            factor = [None]

            def scale():
                factor[0] = factor_of()

            def renew(block):
                rows = rows_at(block, features)
                gain = out_cols[rows, l : l + 1]
                change = branch_all[l, rows, :].astype(F32) * factor[0] * gain
                h_all[l + 1, rows, :] = (h_all[l, rows, :].astype(F32) + change).astype(BF16)

            def branch_hook(i):
                if i == stream_pieces:
                    following[1][0].relay()
                    following[0][0].relay()
                if i == stream_pieces + 2:
                    following[1][1].relay()
                    following[0][1].relay()
                    for part in out_proj[l + 1]:
                        part.send_y()

            drain(branch_spread, scale, renew, branch_hook)

    for copy, condition in sent:
        if condition is None:
            copy.wait_send()
        else:
            pl.when(condition)(copy.wait_send)
    assert counter[0] <= send_sem.shape[0]
    assert local_count[0] <= local_sem.shape[0]


def copies_of(ny, nx, nz, layers, features, channels):
    n_sp, n_tp = ny * nx, 2 * nz
    stream_pieces = pieces_of(features, 128)
    groups = pieces_of(channels, LANES)
    conv_pieces = groups * pieces_of(channels // groups, 64)
    spread = 4 * (nz - 1) + 1
    weights = 2 * (ny - 1) + (n_sp - 1) * (4 * (layers - 1) + stream_pieces * layers)
    cross = (2 * nz - 1) * stream_pieces * 2 * (nx - 1)
    spreads = spread * (stream_pieces * layers + conv_pieces * layers)
    small = (n_tp - 1) * (2 + 2 * layers) + groups * (nx - 1) + 2 * groups * layers
    return weights + cross + spreads + small


def on_device(n_sp, n_tp, stream, value_weight, gate_weight, conv_taps, norm_gain, out_weight, out_gain):
    layers, channels, f_cols = value_weight.shape
    features, positions = stream.shape
    c_cols = out_weight.shape[2]
    ny, nx = grid_of(n_sp)
    copies = copies_of(ny, nx, n_tp // 2, layers, features, channels)
    vmem = pl.BlockSpec(memory_space=pltpu.VMEM)
    hbm = pl.BlockSpec(memory_space=pl.ANY)
    return pl.pallas_call(
        functools.partial(kernel, n_sp, n_tp, layers),
        out_shape=jax.ShapeDtypeStruct(stream.shape, BF16),
        in_specs=[hbm, hbm, hbm, vmem, vmem, hbm, vmem],
        out_specs=vmem,
        scratch_shapes=[
            pltpu.VMEM((layers, n_tp * features, positions), BF16),
            pltpu.VMEM((nx - 1, n_tp * features // nx, positions), BF16),
            pltpu.VMEM((layers, n_tp * channels, positions), BF16),
            pltpu.VMEM((max(layers - 1, 1), n_tp * features, positions), BF16),
            pltpu.VMEM((n_tp * channels, positions), BF16),
            pltpu.VMEM((layers, n_sp, channels, f_cols), BF16),
            pltpu.VMEM((layers, n_sp, channels, f_cols), BF16),
            pltpu.VMEM((layers, n_sp, features, c_cols), BF16),
            pltpu.VMEM((nx - 1, 2, channels, positions), BF16),
            pltpu.VMEM((nx - 1, 2, channels, positions), BF16),
            pltpu.VMEM((layers, positions + 2 * EDGE, channels), F32),
            pltpu.VMEM((positions, channels), F32),
            pltpu.VMEM((layers, 2 * EDGE, channels), F32),
            pltpu.VMEM((2, channels, positions), F32),
            pltpu.VMEM((layers, n_tp, 2, positions), F32),
            pltpu.VMEM((layers, n_tp, 1, positions), F32),
            pltpu.VMEM((n_tp, layers, channels), BF16),
            pltpu.VMEM((n_tp, layers, features), BF16),
            pltpu.VMEM((n_tp * channels, 8), F32),
            pltpu.VMEM((n_tp * features, 8), F32),
            pltpu.SemaphoreType.DMA((layers * (4 + 2 * pieces_of(features, 128)) + 1,)),
            pltpu.SemaphoreType.DMA((copies,)),
            pltpu.SemaphoreType.DMA((copies,)),
        ],
        compiler_params=pltpu.CompilerParams(
            collective_id=0, has_side_effects=True, vmem_limit_bytes=60 * 1024 * 1024
        ),
    )(stream, value_weight, gate_weight, conv_taps, norm_gain, out_weight, out_gain)


def solution(mesh):
    return jax.shard_map(
        functools.partial(on_device, mesh.shape["sp"], mesh.shape["tp"]),
        mesh=mesh,
        in_specs=(
            P("tp", "sp"),
            P(None, "tp", "sp"),
            P(None, "tp", "sp"),
            P(None, "tp", None),
            P(None, "tp"),
            P(None, "tp", "sp"),
            P(None, "tp"),
        ),
        out_specs=P("tp", "sp"),
        check_vma=False,
    )
```

```python
import functools

import jax
import jax.numpy as jnp
from jax import lax
from jax.experimental import pallas as pl
from jax.experimental.pallas import tpu as pltpu
from jax.sharding import PartitionSpec as P

MESH = pl.DeviceIdType.MESH
F32 = jnp.float32
BF16 = jnp.bfloat16
LANES = 128
EDGE = 16
TILE = 64


def grid_of(count):
    nx = int(count**0.5)
    while count % nx:
        nx -= 1
    return count // nx, nx


def pieces_of(rows, size):
    return max(1, rows // size)


def cuts_of(positions):
    inner = positions - 2 * EDGE
    count = max(1, inner // 64)
    size = inner // count // EDGE * EDGE
    cuts = [(EDGE + k * size, size) for k in range(count - 1)]
    first = EDGE + (count - 1) * size
    cuts.append((first, positions - EDGE - first))
    return cuts


def kernel(
    n_sp, n_tp, n_layers,
    stream, value_w, gate_w, taps, norm_gain, out_w, out_gain,
    result,
    h_all, x_all, conv_all, conv_edge, branch_all, active, v_buf, g_buf, o_buf, part_out, part_in, wide, stat_cols, tap_rows,
    acc, sums, squares, norm_rows, out_rows, out_cols,
    local_sem, send_sem, recv_sem,
):
    ny, nx = grid_of(n_sp)
    nz = n_tp // 2
    s, t = lax.axis_index("sp"), lax.axis_index("tp")
    y, x = s // nx, s % nx
    z, c = t // 2, t % 2
    features, positions = stream.shape
    channels = value_w.shape[1]
    f_cols = value_w.shape[2]
    c_cols = out_w.shape[2]
    width = channels * n_tp
    model = features * n_tp
    n_taps = taps.shape[0]
    reach = n_taps // 2
    groups = pieces_of(channels, LANES)
    group = channels // groups
    sends, recvs, sent = [0], [0], []

    def send_slot():
        sends[0] += 1
        return sends[0] - 1

    def recv_slot(count=1):
        recvs[0] += count
        return recvs[0] - count

    def remote(src, dst, sp, tp, send=None, recv=None):
        return pltpu.make_async_remote_copy(
            src_ref=src, dst_ref=dst,
            send_sem=send_sem.at[0 if send is None else send], recv_sem=recv_sem.at[0 if recv is None else recv],
            device_id={"sp": sp, "tp": tp}, device_id_type=MESH,
        )

    def start(copy, condition=None):
        if condition is None:
            copy.start()
        else:
            pl.when(condition)(copy.start)

    def leave(ref, send, condition=None):
        sent.append((remote(ref, ref, s, t, send=send), condition))

    def slot_of(k, j):
        return lax.rem(y + ny - k, ny) * nx + lax.rem(x + nx - j, nx)

    def x_peer(j):
        return y * nx + lax.rem(x + j, nx)

    def y_peer(k):
        return lax.rem(y + k, ny) * nx + x

    local_count = [0]

    def local_copy(src, dst):
        i = local_count[0]
        local_count[0] += 1
        copy = pltpu.make_async_copy(src, dst, local_sem.at[i])
        copy.start()
        return copy

    class Gather:
        def __init__(self, src, dst, x_first, whole, send):
            self.copies, self.own_x, self.own_y, self.relays = {}, [], [], []
            for k in range(ny):
                for j in range(nx if whole else 1):
                    if k == 0 and j == 0:
                        continue
                    if x_first:
                        along_x = k == 0
                        origin = (0, 0) if along_x else (0, j)
                    else:
                        along_x = j > 0
                        origin = (k, 0) if along_x else (0, 0)
                    own = origin == (0, 0)
                    target = x_peer(j) if along_x else y_peer(k)
                    origin_slot = slot_of(*origin)
                    copy = remote(
                        src if own else dst(origin_slot), dst(origin_slot), target, t, send=send, recv=recv_slot()
                    )
                    self.copies[k, j] = copy
                    if not own:
                        self.relays.append((copy, origin))
                    elif along_x:
                        self.own_x.append(copy)
                    else:
                        self.own_y.append(copy)
            self.local = local_copy(src, dst(s))
            self.here, self.done = set(), set()

        def once(self, name):
            fresh = name not in self.done
            self.done.add(name)
            return fresh

        def send_x(self):
            if self.once("x"):
                for copy in self.own_x:
                    start(copy)

        def send_y(self):
            if self.once("y"):
                for copy in self.own_y:
                    start(copy)

        def relay(self):
            if self.once("relay"):
                for copy, origin in self.relays:
                    self.arrive(*origin)
                    start(copy)

        def flush(self):
            self.send_x()
            self.send_y()
            self.relay()

        def arrive(self, k, j):
            if (k, j) not in self.here:
                self.here.add((k, j))
                if k == 0 and j == 0:
                    self.local.wait()
                else:
                    self.copies[k, j].wait_recv()

    def gathers(w_ref, buf, l, orders, whole=True):
        rows = w_ref.shape[1] // len(orders)
        made, send = [], send_slot()
        leave(buf.at[l, pl.ds(0, (n_sp if whole else ny) - 1)], send)
        for i, x_first in enumerate(orders):
            part = pl.ds(i * rows, rows)
            made.append(Gather(w_ref.at[l, part], lambda q, part=part: buf.at[l, q, part], x_first, whole, send))
        return made

    class Spread:
        def __init__(self, pieces, at, whole, direct=False):
            def place(zz, cc, k):
                return at(jnp.clip(zz, 0, nz - 1) * 2 + cc, k)

            def full(zz, cc):
                return whole(jnp.clip(zz, 0, nz - 1) * 2 + cc)

            other = z * 2 + 1 - c
            self.pieces, self.place, self.direct = pieces, place, direct
            send, recv = send_slot(), recv_slot()
            self.across = [
                remote(place(z, c, k), place(z, c, k), s, other, send, recv) for k in range(pieces)
            ]
            self.landed = remote(full(z, 1 - c), full(z, 1 - c), s, other, recv=recv)
            leave(full(z, c), send)
            self.along, self.goes, self.hand, self.has, self.handed = {}, {}, {}, {}, {}
            for d in range(1, nz):
                for way in (1, -1):
                    has = (z - way * d >= 0) & (z - way * d < nz)
                    self.has[way, d] = has
                    send, hand_send, hand_recv = send_slot(), send_slot(), recv_slot()
                    if direct:
                        from_z, to_z = z, z + way * d
                        self.goes[way, d] = (to_z >= 0) & (to_z < nz)
                    else:
                        from_z, to_z = z - way * (d - 1), z + way
                        self.goes[way, d] = (from_z >= 0) & (from_z < nz) & (to_z >= 0) & (to_z < nz)
                    target = jnp.clip(to_z, 0, nz - 1) * 2 + c
                    for k in range(pieces):
                        held = place(from_z, c, k)
                        self.along[way, d, k] = remote(held, held, s, target, send, recv_slot())
                        seen = place(z - way * d, c, k)
                        self.hand[way, d, k] = remote(seen, seen, s, other, hand_send, hand_recv)
                    block = full(z - way * d, c)
                    self.handed[way, d] = remote(block, block, s, other, recv=hand_recv)
                    leave(block, send, self.goes[way, d])
                    leave(block, hand_send, has)

        def send(self, way, d, k):
            start(self.along[way, d, k], self.goes[way, d])

        def start_own(self, k):
            for d in range(1, nz) if self.direct else (1,):
                for way in (1, -1):
                    self.send(way, d, k)
            start(self.across[k])

        def step(self, d, k, extra=None):
            for way in (1, -1):
                pl.when(self.has[way, d])(self.along[way, d, k].wait_recv)
                if d + 1 < nz and not self.direct:
                    self.send(way, d + 1, k)
                start(self.hand[way, d, k], self.has[way, d])
                if extra is not None:
                    extra(way, d, k)

        def wait_across(self):
            self.landed.wait_recv()

        def wait_hand(self, way, d):
            self.handed[way, d].wait_recv()

    class Cross:
        def __init__(self, spread):
            self.spread = spread
            self.size = features // spread.pieces
            self.sends, self.base, self.hands = {}, {}, {}

        def facts(self, way, d):
            zz = z - way * d
            ok = (zz >= 0) & (zz < nz)
            q = jnp.clip(zz, 0, nz - 1)
            return ok, q, lax.rem(q, nx)

        def rows(self, q, k, count=1):
            size = self.size
            row = (q // nx * 2 + c) * features + k * size
            return pl.ds(pl.multiple_of(row, size), size * count)

        def forward(self, way, d, k):
            ok, q, owner = self.facts(way, d)
            pick = jnp.clip(lax.rem(owner - x + nx, nx) - 1, 0, nx - 2)
            if (way, d) not in self.sends:
                self.sends[way, d] = send_slot()
                leave(x_all.at[0, self.rows(q, 0, self.spread.pieces), :], self.sends[way, d], ok & (owner != x))
            base = self.base[way, d, k] = recv_slot(nx - 1)
            copy = remote(
                self.spread.place(q, c, k), x_all.at[pick, self.rows(q, k), :], y * nx + owner, t,
                self.sends[way, d], base + pick,
            )
            start(copy, ok & (owner != x))

        def receive(self, way, d, k):
            ok, q, owner = self.facts(way, d)
            mine = ok & (owner == x)
            for j in range(1, nx):
                if k == 0:
                    block = x_all.at[j - 1, self.rows(q, 0, self.spread.pieces), :]
                    send, recv = send_slot(), recv_slot()
                    self.hands[way, d, j] = (send, recv, remote(block, block, s, t, recv=recv), mine)
                    leave(block, send, mine)
                send, recv, _, _ = self.hands[way, d, j]
                here = x_all.at[j - 1, self.rows(q, k), :]
                landed = remote(here, here, s, t, recv=self.base[way, d, k] + j - 1)
                pl.when(mine)(landed.wait_recv)
                start(remote(here, here, s, z * 2 + 1 - c, send, recv), mine)

        def finish(self):
            for _, _, handed, mine in self.hands.values():
                pl.when(mine)(handed.wait_recv)

    def exchange(src, buf):
        send, recv = send_slot(), recv_slot()
        others = buf.at[pl.ds(0, n_tp - 1)]
        for k in range(1, n_tp):
            start(remote(src, buf.at[t], s, lax.rem(t + k, n_tp), send, recv))
        leave(others, send)
        return [remote(others, others, s, t, recv=recv)]

    def arrived(copies):
        for copy in copies:
            copy.wait_recv()

    my_rows = pl.ds(pl.multiple_of(t * features, features), features)
    stream_pieces = pieces_of(features, 128)
    cuts = cuts_of(positions)

    def row_spread(buf):
        size = features // stream_pieces

        def at(block, k):
            return buf.at[pl.ds(pl.multiple_of(block * features + k * size, size), size), :]

        def whole(block):
            return buf.at[pl.ds(pl.multiple_of(block * features, features), features), :]

        return Spread(stream_pieces, at, whole)

    def position_spreads(inner, edge):
        return (
            Spread(
                len(cuts), lambda block, k: inner.at[block, pl.ds(cuts[k][0], cuts[k][1]), :],
                lambda block: inner.at[block, pl.ds(EDGE, positions - 2 * EDGE), :],
            ),
            Spread(1, lambda block, k: edge.at[block], lambda block: edge.at[block], direct=True),
        )

    stream_copy = local_copy(stream, h_all.at[0, my_rows, :])
    barrier = pltpu.get_barrier_semaphore()
    for k in range(1, n_sp):
        pl.semaphore_signal(
            barrier, inc=1, device_id={"sp": lax.rem(s + k, n_sp), "tp": t}, device_id_type=MESH
        )
    for k in range(1, n_tp):
        pl.semaphore_signal(
            barrier, inc=1, device_id={"sp": s, "tp": lax.rem(t + k, n_tp)}, device_id_type=MESH
        )
    in_proj, out_proj = [], []
    out_parts = pieces_of(features, 128)
    for l in range(n_layers):
        if l == 0:
            v_parts = gathers(value_w, v_buf, l, [True], whole=False)
            g_parts = gathers(gate_w, g_buf, l, [True], whole=False)
        else:
            v_parts = gathers(value_w, v_buf, l, [True, True])
            g_parts = gathers(gate_w, g_buf, l, [False, False])
        in_proj.append((v_parts, g_parts))
        last = l + 1 == n_layers
        out_proj.append(gathers(out_w, o_buf, l, [last] * out_parts))
    norm_rows[t] = norm_gain[...]
    out_rows[t] = out_gain[...]
    for l in range(n_layers):
        tap_rows[l, 0:n_taps, :] = taps[:, l, :].astype(F32)
    stream_copy.wait()
    pl.semaphore_wait(barrier, n_sp + n_tp - 2)

    spread = row_spread(h_all.at[0])
    cross = Cross(spread)
    for k in range(stream_pieces):
        spread.start_own(k)
        cross.forward(1, 0, k)
    for part in in_proj[0][0] + in_proj[0][1]:
        part.send_y()
    out_proj[0][0].send_x()
    gain_copies = exchange(norm_gain, norm_rows) + exchange(out_gain, out_rows)

    def turn_gain(i):
        rows = out_rows[i].astype(F32)
        fill = jnp.zeros((8 - n_layers, features), F32)
        out_cols[i * features : (i + 1) * features, :] = jnp.concatenate([rows, fill], axis=0).T

    def across_lanes(a, b):
        return lax.dot_general(a, b, (((1,), (1,)), ((), ())), preferred_element_type=F32)

    turned = [0]
    steps = [(k, j) for k in range(ny) for j in range(nx)]
    right, left = lax.rem(s + 1, n_sp), lax.rem(s + n_sp - 1, n_sp)
    has_right, has_left = s < n_sp - 1, s > 0

    def rows_at(q, count):
        return pl.ds(pl.multiple_of(q * count, count), count)

    for l in range(n_layers):
        last = l + 1 == n_layers
        following = None if last else in_proj[l + 1]
        groups_of_rows = [pl.ds(m * group, group) for m in range(groups)]
        if l == 0:
            waiting = list(out_proj[0][1:])
            for d in range(1, nz):
                for k in range(stream_pieces):
                    spread.step(d, k, cross.forward)
                    for way in ((1,) if d == 1 else (1, -1)):
                        cross.receive(way, d - 1, k)
                    if waiting and ((d - 1) * stream_pieces + k) % 2 == 1:
                        waiting.pop(0).send_x()
            for part in waiting:
                part.send_x()
            spread.wait_across()
            for d in range(1, nz):
                for way in (1, -1):
                    @pl.when(spread.has[way, d])
                    def _():
                        spread.wait_hand(way, d)
            for half, (parts, buf) in enumerate(zip(in_proj[l], (v_buf, g_buf))):
                total = None
                for k in range(ny):
                    for part in parts:
                        part.arrive(k, 0)
                    slot = slot_of(k, 0)
                    one = jnp.dot(buf[l, slot], h_all[l, rows_at(slot, f_cols), :], preferred_element_type=F32)
                    total = one if total is None else total + one
                acc[half] = total
            for k in range(stream_pieces):
                for way in (1, -1):
                    cross.receive(way, nz - 1, k)
            cross.finish()
            part_copies = {}
            for m, rows in enumerate(groups_of_rows):
                for j in range(1, nx):
                    for half, buf in enumerate((v_buf, g_buf)):
                        total = None
                        for k in range(ny):
                            block = rows_at(lax.rem(y + ny - k, ny), f_cols)
                            one = jnp.dot(
                                buf[l, slot_of(k, 0), rows, :], x_all[j - 1, block, :],
                                preferred_element_type=F32,
                            )
                            total = one if total is None else total + one
                        part_out[j - 1, half, rows, :] = total.astype(BF16)
                    mine = part_out.at[j - 1, :, rows, :]
                    send = send_slot()
                    copy = remote(
                        mine, part_in.at[j - 1, :, rows, :], y * nx + lax.rem(x + nx - j, nx), t,
                        send, recv_slot(),
                    )
                    start(copy)
                    leave(mine, send)
                    part_copies[m, j] = copy
            for part in out_proj[0]:
                part.send_y()
        else:
            for part in in_proj[l][0] + in_proj[l][1]:
                part.flush()
            for k, j in steps:
                slot = slot_of(k, j)
                for half, (parts, buf) in enumerate(zip(in_proj[l], (v_buf, g_buf))):
                    for part in parts:
                        part.arrive(k, j)
                    one = jnp.dot(buf[l, slot], h_all[l, rows_at(slot, f_cols), :], preferred_element_type=F32)
                    if (k, j) == (0, 0):
                        acc[half] = one
                    else:
                        acc[half] += one

        edges = []
        for m, rows in enumerate(groups_of_rows):
            lanes = pl.ds(m * group, group)
            value, gate = acc[0, rows, :], acc[1, rows, :]
            if l == 0:
                for j in range(1, nx):
                    part_copies[m, j].wait_recv()
                    value = value + part_in[j - 1, 0, rows, :].astype(F32)
                    gate = gate + part_in[j - 1, 1, rows, :].astype(F32)
            gated = (value * jax.nn.sigmoid(gate)).astype(BF16)
            wide[l, pl.ds(EDGE, positions), lanes] = gated.astype(F32).T
            pair = []
            for first, land, peer, here in (
                (positions, 0, right, has_right), (EDGE, EDGE + positions, left, has_left)
            ):
                mine, send = wide.at[l, pl.ds(first, EDGE), lanes], send_slot()
                copy = remote(mine, wide.at[l, pl.ds(land, EDGE), lanes], peer, t, send, recv_slot())
                start(copy, here)
                leave(mine, send, here)
                pair.append(copy)
            to_right, to_left = pair
            edges.append((to_right, to_left))

        if l == 0:
            if following is not None:
                following[0][0].send_x()
                for part in following[1] + following[0]:
                    part.send_y()
        if last:
            for part in out_proj[l]:
                part.send_x()

        blank = jnp.zeros((EDGE, channels), F32)

        @pl.when(s == 0)
        def _():
            wide[l, 0:EDGE, :] = blank

        @pl.when(s == n_sp - 1)
        def _():
            wide[l, EDGE + positions : 2 * EDGE + positions, :] = blank

        def convolve(first, count, dst, land):
            while count:
                size = min(TILE, count)
                for m in range(groups):
                    lanes = pl.ds(m * group, group)
                    extent = size + 2 * EDGE
                    window = wide[l, pl.ds(first, extent), lanes]
                    total = None
                    for r in range(8):
                        moved = window if r == 0 else pltpu.roll(window, extent - r, 0)
                        for q in range(0, 2 * EDGE + 1, 8):
                            tap = q + r - (EDGE - reach)
                            if 0 <= tap < n_taps:
                                term = tap_rows[l, tap : tap + 1, lanes] * moved[q : q + size]
                                total = term if total is None else total + term
                    dst[l, t, pl.ds(land, size), lanes] = total.astype(BF16)
                first, land, count = first + size, land + size, count - size

        def total_up(phase, seen):
            square = seen.astype(F32) * seen.astype(F32)
            high = square.astype(BF16)
            low = (square - high.astype(F32)).astype(BF16)
            ones = jnp.ones((8, channels), BF16)
            sums[l, phase, t, 0:1, :] = across_lanes(ones, seen)[0:1]
            sums[l, phase, t, 1:2, :] = (across_lanes(ones, high) + across_lanes(ones, low))[0:1]
            return exchange(sums.at[l, phase, t], sums.at[l, phase])

        inner, edge = position_spreads(conv_all.at[l], conv_edge.at[l])
        border = jnp.zeros((EDGE, channels), BF16)
        conv_all[l, t, 0:EDGE, :] = border
        conv_all[l, t, positions - EDGE : positions, :] = border
        for k, (first, count) in enumerate(cuts):
            convolve(first, count, conv_all, first)
            inner.start_own(k)
        sum_copies = [total_up(0, conv_all[l, t]), None]

        def finish_edges():
            for to_right, to_left in edges:
                pl.when(has_left)(to_right.wait_recv)
                pl.when(has_right)(to_left.wait_recv)
            convolve(0, EDGE, conv_edge, 0)
            convolve(positions - EDGE, EDGE, conv_edge, EDGE)
            edge.start_own(0)
            conv_all[l, t, 0:EDGE, :] = conv_edge[l, t, 0:EDGE, :]
            conv_all[l, t, positions - EDGE : positions, :] = conv_edge[l, t, EDGE : 2 * EDGE, :]
            sum_copies[1] = total_up(1, conv_all[l, t])

        def settle(phase):
            arrived(sum_copies[phase])
            totals = jnp.sum(sums[l, phase], axis=0)
            average = totals[0:1] / width
            variance = totals[1:2] / width - average * average
            for i, row in enumerate((average, lax.rsqrt(variance + 1e-05))):
                column = jnp.broadcast_to(row, (LANES, positions)).T
                if channels > LANES:
                    column = jnp.concatenate([column] * (channels // LANES), axis=1)
                stat_cols[i] = column[:, :channels]

        def activate(src, block, first, count, land):
            gain = norm_rows[block].astype(F32)[l : l + 1]
            place = pl.ds(land, count)
            seen = src[l, block, pl.ds(first, count), :].astype(F32)
            scaled = (seen - stat_cols[0, place, :]) * stat_cols[1, place, :] * gain
            active[block, place, :] = (scaled / (1.0 + jnp.exp(-scaled))).astype(BF16)

        def activate_inner(block):
            activate(conv_all, block, EDGE, positions - 2 * EDGE, EDGE)

        def drain(spread, ready, consume, hook, finish=None):
            def take(d):
                for way in (1, -1):
                    @pl.when(spread.has[way, d])
                    def _():
                        consume((z - way * d) * 2 + c)
                        spread.wait_hand(way, d)
                        consume((z - way * d) * 2 + 1 - c)

            when = min(2, nz - 1)
            for d in range(1, nz):
                for k in range(spread.pieces):
                    spread.step(d, k)
                    hook((d - 1) * spread.pieces + k)
                if d == when:
                    ready()
                    consume(t)
                    spread.wait_across()
                    consume(z * 2 + 1 - c)
                if d >= when and d > 1:
                    take(d - 1)
            if finish is not None:
                finish()
            take(nz - 1)

        def conv_hook(i):
            if i == min(1, len(cuts) - 1):
                finish_edges()
            if l == 0:
                if i == 2:
                    arrived(gain_copies)
                if i >= 2 and turned[0] < n_tp:
                    turn_gain(turned[0])
                    turned[0] += 1
                if i == 1:
                    for part in out_proj[l][: out_parts // 2]:
                        part.relay()
                if i == 4:
                    for part in out_proj[l][out_parts // 2 :]:
                        part.relay()
                if i == 5 and following is not None:
                    following[0][1].send_x()
            if last and i % 3 == 0 and 0 < i // 3 <= out_parts:
                out_proj[l][i // 3 - 1].flush()

        def catch_edges():
            for d in range(1, nz):
                edge.step(d, 0)

        drain(inner, lambda: settle(0), activate_inner, conv_hook, catch_edges)
        edge.wait_across()
        for d in range(1, nz):
            for way in (1, -1):
                @pl.when(edge.has[way, d])
                def _():
                    edge.wait_hand(way, d)
        settle(1)
        for block in range(n_tp):
            activate(conv_edge, block, 0, EDGE, 0)
            activate(conv_edge, block, EDGE, EDGE, positions - EDGE)
        while turned[0] < n_tp:
            turn_gain(turned[0])
            turned[0] += 1
        for part in out_proj[l]:
            part.flush()
        total = None
        for k, j in steps:
            slot = slot_of(k, j)
            for part in out_proj[l]:
                part.arrive(k, j)
            for i in range(c_cols // channels):
                one = across_lanes(
                    o_buf[l, slot, :, i * channels : (i + 1) * channels], active[slot * (c_cols // channels) + i]
                )
                total = one if total is None else total + one
        narrow_branch = total.astype(BF16)
        branch = narrow_branch.astype(F32)
        squares[l, t, 0:1, :] = jnp.sum(branch * branch, axis=0, keepdims=True)
        square_copies = exchange(squares.at[l, t], squares.at[l])

        def factor_of():
            arrived(square_copies)
            return lax.rsqrt(jnp.sum(squares[l], axis=0) / model + 1e-06)

        if last:
            factor = factor_of()
            gain = out_cols[my_rows, l : l + 1]
            fresh = h_all[l, my_rows, :].astype(F32) + branch * factor * gain
            result[...] = fresh.astype(BF16)
        else:
            branch_all[l, my_rows, :] = narrow_branch
            branch_spread = row_spread(branch_all.at[l])
            for k in range(stream_pieces):
                branch_spread.start_own(k)
            if l == 0:
                for part in following[0] + following[1]:
                    part.send_x()

            factor = [None]

            def scale():
                factor[0] = factor_of()

            def renew(block):
                rows = rows_at(block, features)
                gain = out_cols[rows, l : l + 1]
                change = branch_all[l, rows, :].astype(F32) * factor[0] * gain
                h_all[l + 1, rows, :] = (h_all[l, rows, :].astype(F32) + change).astype(BF16)

            def branch_hook(i):
                if i == stream_pieces:
                    following[1][0].relay()
                    following[0][0].relay()
                if i == stream_pieces + 2:
                    following[1][1].relay()
                    following[0][1].relay()
                    for part in out_proj[l + 1]:
                        part.send_y()

            drain(branch_spread, scale, renew, branch_hook)

    for copy, condition in sent:
        if condition is None:
            copy.wait_send()
        else:
            pl.when(condition)(copy.wait_send)
    assert sends[0] == send_sem.shape[0], sends
    assert recvs[0] == recv_sem.shape[0], recvs
    assert local_count[0] == local_sem.shape[0], local_count


def slots_of(ny, nx, nz, layers, features, channels, positions):
    n_sp, far = ny * nx, 2 * (nz - 1)
    pieces, cuts, groups = pieces_of(features, 128), len(cuts_of(positions)), pieces_of(channels, LANES)
    small = 2 + 3 * layers + groups * (nx - 1) + 2 * groups * layers
    send = 3 * layers * (1 + 2 * far) + (far + 1) * nx + 3 * layers + small
    recv = layers * (3 + far * (pieces + 1 + cuts + 1 + 2)) + (far + 1) * (pieces + 1) * (nx - 1)
    recv += 2 * (ny - 1) + (n_sp - 1) * (4 * (layers - 1) + pieces * layers) + small
    local = 1 + 2 + 4 * (layers - 1) + pieces * layers
    return send, recv, local


def on_device(n_sp, n_tp, stream, value_weight, gate_weight, conv_taps, norm_gain, out_weight, out_gain):
    layers, channels, f_cols = value_weight.shape
    features, positions = stream.shape
    c_cols = out_weight.shape[2]
    ny, nx = grid_of(n_sp)
    send, recv, local = slots_of(ny, nx, n_tp // 2, layers, features, channels, positions)
    vmem = pl.BlockSpec(memory_space=pltpu.VMEM)
    hbm = pl.BlockSpec(memory_space=pl.ANY)
    return pl.pallas_call(
        functools.partial(kernel, n_sp, n_tp, layers),
        out_shape=jax.ShapeDtypeStruct(stream.shape, BF16),
        in_specs=[hbm, hbm, hbm, vmem, vmem, hbm, vmem],
        out_specs=vmem,
        scratch_shapes=[
            pltpu.VMEM((layers, n_tp * features, positions), BF16),
            pltpu.VMEM((nx - 1, n_tp * features // nx, positions), BF16),
            pltpu.VMEM((layers, n_tp, positions, channels), BF16),
            pltpu.VMEM((layers, n_tp, 2 * EDGE, channels), BF16),
            pltpu.VMEM((max(layers - 1, 1), n_tp * features, positions), BF16),
            pltpu.VMEM((n_tp, positions, channels), BF16),
            pltpu.VMEM((layers, n_sp, channels, f_cols), BF16),
            pltpu.VMEM((layers, n_sp, channels, f_cols), BF16),
            pltpu.VMEM((layers, n_sp, features, c_cols), BF16),
            pltpu.VMEM((nx - 1, 2, channels, positions), BF16),
            pltpu.VMEM((nx - 1, 2, channels, positions), BF16),
            pltpu.VMEM((layers, positions + 2 * EDGE, channels), F32),
            pltpu.VMEM((2, positions, channels), F32),
            pltpu.VMEM((layers, 2 * EDGE, channels), F32),
            pltpu.VMEM((2, channels, positions), F32),
            pltpu.VMEM((layers, 2, n_tp, 2, positions), F32),
            pltpu.VMEM((layers, n_tp, 1, positions), F32),
            pltpu.VMEM((n_tp, layers, channels), BF16),
            pltpu.VMEM((n_tp, layers, features), BF16),
            pltpu.VMEM((n_tp * features, 8), F32),
            pltpu.SemaphoreType.DMA((local,)),
            pltpu.SemaphoreType.DMA((send,)),
            pltpu.SemaphoreType.DMA((recv,)),
        ],
        compiler_params=pltpu.CompilerParams(
            collective_id=0, has_side_effects=True, vmem_limit_bytes=60 * 1024 * 1024
        ),
    )(stream, value_weight, gate_weight, jnp.transpose(conv_taps, (2, 0, 1)), norm_gain, out_weight, out_gain)


def solution(mesh):
    return jax.shard_map(
        functools.partial(on_device, mesh.shape["sp"], mesh.shape["tp"]),
        mesh=mesh,
        in_specs=(
            P("tp", "sp"),
            P(None, "tp", "sp"),
            P(None, "tp", "sp"),
            P(None, "tp", None),
            P(None, "tp"),
            P(None, "tp", "sp"),
            P(None, "tp"),
        ),
        out_specs=P("tp", "sp"),
        check_vma=False,
    )
```

```python
import functools

import jax
import jax.numpy as jnp
from jax import lax
from jax.experimental import pallas as pl
from jax.experimental.pallas import tpu as pltpu
from jax.sharding import PartitionSpec as P

MESH = pl.DeviceIdType.MESH
F32 = jnp.float32
BF16 = jnp.bfloat16
LANES = 128
EDGE = 16
TILE = 64


def grid_of(count):
    nx = int(count**0.5)
    while count % nx:
        nx -= 1
    return count // nx, nx


def pieces_of(rows, size):
    return max(1, rows // size)


def cuts_of(positions):
    inner = positions - 2 * EDGE
    count = max(1, inner // 64)
    size = inner // count // EDGE * EDGE
    cuts = [(EDGE + k * size, size) for k in range(count - 1)]
    first = EDGE + (count - 1) * size
    cuts.append((first, positions - EDGE - first))
    return cuts


def kernel(
    n_sp, n_tp, n_layers,
    stream, value_w, gate_w, taps, norm_gain, out_w, out_gain,
    result,
    h_all, x_all, x_branch, own_factor, peer_factor, conv_all, conv_edge, branch_all, active, v_buf, g_buf, o_buf, part_out, part_in, wide, stat_cols, tap_rows,
    acc, sums, squares, norm_rows, out_rows, out_cols,
    local_sem, send_sem, recv_sem,
):
    ny, nx = grid_of(n_sp)
    nz = n_tp // 2
    s, t = lax.axis_index("sp"), lax.axis_index("tp")
    y, x = s // nx, s % nx
    z, c = t // 2, t % 2
    features, positions = stream.shape
    channels = value_w.shape[1]
    f_cols = value_w.shape[2]
    c_cols = out_w.shape[2]
    width = channels * n_tp
    model = features * n_tp
    n_taps = taps.shape[0]
    reach = n_taps // 2
    groups = pieces_of(channels, LANES)
    group = channels // groups
    sends, recvs, sent = [0], [0], []

    def send_slot():
        sends[0] += 1
        return sends[0] - 1

    def recv_slot(count=1):
        recvs[0] += count
        return recvs[0] - count

    def remote(src, dst, sp, tp, send=None, recv=None):
        return pltpu.make_async_remote_copy(
            src_ref=src, dst_ref=dst,
            send_sem=send_sem.at[0 if send is None else send], recv_sem=recv_sem.at[0 if recv is None else recv],
            device_id={"sp": sp, "tp": tp}, device_id_type=MESH,
        )

    def start(copy, condition=None):
        if condition is None:
            copy.start()
        else:
            pl.when(condition)(copy.start)

    def leave(ref, send, condition=None):
        sent.append((remote(ref, ref, s, t, send=send), condition))

    def slot_of(k, j):
        return lax.rem(y + ny - k, ny) * nx + lax.rem(x + nx - j, nx)

    def x_peer(j):
        return y * nx + lax.rem(x + j, nx)

    def y_peer(k):
        return lax.rem(y + k, ny) * nx + x

    local_count = [0]

    def local_copy(src, dst):
        i = local_count[0]
        local_count[0] += 1
        copy = pltpu.make_async_copy(src, dst, local_sem.at[i])
        copy.start()
        return copy

    class Gather:
        def __init__(self, src, dst, x_first, whole, send):
            self.copies, self.own_x, self.own_y, self.relays = {}, [], [], []
            for k in range(ny):
                for j in range(nx if whole else 1):
                    if k == 0 and j == 0:
                        continue
                    if x_first:
                        along_x = k == 0
                        origin = (0, 0) if along_x else (0, j)
                    else:
                        along_x = j > 0
                        origin = (k, 0) if along_x else (0, 0)
                    own = origin == (0, 0)
                    target = x_peer(j) if along_x else y_peer(k)
                    origin_slot = slot_of(*origin)
                    copy = remote(
                        src if own else dst(origin_slot), dst(origin_slot), target, t, send=send, recv=recv_slot()
                    )
                    self.copies[k, j] = copy
                    if not own:
                        self.relays.append((copy, origin))
                    elif along_x:
                        self.own_x.append(copy)
                    else:
                        self.own_y.append(copy)
            self.local = local_copy(src, dst(s))
            self.here, self.done = set(), set()

        def once(self, name):
            fresh = name not in self.done
            self.done.add(name)
            return fresh

        def send_x(self):
            if self.once("x"):
                for copy in self.own_x:
                    start(copy)

        def send_y(self):
            if self.once("y"):
                for copy in self.own_y:
                    start(copy)

        def relay(self):
            if self.once("relay"):
                for copy, origin in self.relays:
                    self.arrive(*origin)
                    start(copy)

        def flush(self):
            self.send_x()
            self.send_y()
            self.relay()

        def arrive(self, k, j):
            if (k, j) not in self.here:
                self.here.add((k, j))
                if k == 0 and j == 0:
                    self.local.wait()
                else:
                    self.copies[k, j].wait_recv()

    def gathers(w_ref, buf, l, orders, whole=True):
        rows = w_ref.shape[1] // len(orders)
        made, send = [], send_slot()
        leave(buf.at[l, pl.ds(0, (n_sp if whole else ny) - 1)], send)
        for i, x_first in enumerate(orders):
            part = pl.ds(i * rows, rows)
            made.append(Gather(w_ref.at[l, part], lambda q, part=part: buf.at[l, q, part], x_first, whole, send))
        return made

    class Spread:
        def __init__(self, pieces, at, whole, direct=False):
            def place(zz, cc, k):
                return at(jnp.clip(zz, 0, nz - 1) * 2 + cc, k)

            def full(zz, cc):
                return whole(jnp.clip(zz, 0, nz - 1) * 2 + cc)

            other = z * 2 + 1 - c
            self.pieces, self.place, self.direct = pieces, place, direct
            send, recv = send_slot(), recv_slot()
            self.across = [
                remote(place(z, c, k), place(z, c, k), s, other, send, recv) for k in range(pieces)
            ]
            self.landed = remote(full(z, 1 - c), full(z, 1 - c), s, other, recv=recv)
            leave(full(z, c), send)
            self.along, self.goes, self.hand, self.has, self.handed = {}, {}, {}, {}, {}
            for d in range(1, nz):
                for way in (1, -1):
                    has = (z - way * d >= 0) & (z - way * d < nz)
                    self.has[way, d] = has
                    send, hand_send, hand_recv = send_slot(), send_slot(), recv_slot()
                    if direct:
                        from_z, to_z = z, z + way * d
                        self.goes[way, d] = (to_z >= 0) & (to_z < nz)
                    else:
                        from_z, to_z = z - way * (d - 1), z + way
                        self.goes[way, d] = (from_z >= 0) & (from_z < nz) & (to_z >= 0) & (to_z < nz)
                    target = jnp.clip(to_z, 0, nz - 1) * 2 + c
                    for k in range(pieces):
                        held = place(from_z, c, k)
                        self.along[way, d, k] = remote(held, held, s, target, send, recv_slot())
                        seen = place(z - way * d, c, k)
                        self.hand[way, d, k] = remote(seen, seen, s, other, hand_send, hand_recv)
                    block = full(z - way * d, c)
                    self.handed[way, d] = remote(block, block, s, other, recv=hand_recv)
                    leave(block, send, self.goes[way, d])
                    leave(block, hand_send, has)

        def send(self, way, d, k):
            start(self.along[way, d, k], self.goes[way, d])

        def start_own(self, k):
            for d in range(1, nz) if self.direct else (1,):
                for way in (1, -1):
                    self.send(way, d, k)
            start(self.across[k])

        def step(self, d, k, extra=None):
            for way in (1, -1):
                pl.when(self.has[way, d])(self.along[way, d, k].wait_recv)
                if d + 1 < nz and not self.direct:
                    self.send(way, d + 1, k)
                start(self.hand[way, d, k], self.has[way, d])
                if extra is not None:
                    extra(way, d, k)

        def wait_across(self):
            self.landed.wait_recv()

        def wait_hand(self, way, d):
            self.handed[way, d].wait_recv()

    class Cross:
        def __init__(self, spread, land):
            self.spread, self.land = spread, land
            self.size = features // spread.pieces
            self.sends, self.base, self.hands = {}, {}, {}

        def facts(self, way, d):
            zz = z - way * d
            ok = (zz >= 0) & (zz < nz)
            q = jnp.clip(zz, 0, nz - 1)
            return ok, q, lax.rem(q, nx)

        def rows(self, q, k, count=1):
            size = self.size
            row = (q // nx * 2 + c) * features + k * size
            return pl.ds(pl.multiple_of(row, size), size * count)

        def forward(self, way, d, k):
            ok, q, owner = self.facts(way, d)
            pick = jnp.clip(lax.rem(owner - x + nx, nx) - 1, 0, nx - 2)
            if (way, d) not in self.sends:
                self.sends[way, d] = send_slot()
                leave(self.land.at[0, self.rows(q, 0, self.spread.pieces), :], self.sends[way, d], ok & (owner != x))
            base = self.base[way, d, k] = recv_slot(nx - 1)
            copy = remote(
                self.spread.place(q, c, k), self.land.at[pick, self.rows(q, k), :], y * nx + owner, t,
                self.sends[way, d], base + pick,
            )
            start(copy, ok & (owner != x))

        def receive(self, way, d, k):
            ok, q, owner = self.facts(way, d)
            mine = ok & (owner == x)
            for j in range(1, nx):
                if k == 0:
                    block = self.land.at[j - 1, self.rows(q, 0, self.spread.pieces), :]
                    send, recv = send_slot(), recv_slot()
                    self.hands[way, d, j] = (send, recv, remote(block, block, s, t, recv=recv), mine)
                    leave(block, send, mine)
                send, recv, _, _ = self.hands[way, d, j]
                here = self.land.at[j - 1, self.rows(q, k), :]
                landed = remote(here, here, s, t, recv=self.base[way, d, k] + j - 1)
                pl.when(mine)(landed.wait_recv)
                start(remote(here, here, s, z * 2 + 1 - c, send, recv), mine)

        def finish(self):
            for _, _, handed, mine in self.hands.values():
                pl.when(mine)(handed.wait_recv)

    def exchange(src, buf):
        send, recv = send_slot(), recv_slot()
        others = buf.at[pl.ds(0, n_tp - 1)]
        for k in range(1, n_tp):
            start(remote(src, buf.at[t], s, lax.rem(t + k, n_tp), send, recv))
        leave(others, send)
        return [remote(others, others, s, t, recv=recv)]

    def arrived(copies):
        for copy in copies:
            copy.wait_recv()

    my_rows = pl.ds(pl.multiple_of(t * features, features), features)
    stream_pieces = pieces_of(features, 128)
    cuts = cuts_of(positions)

    def row_spread(buf):
        size = features // stream_pieces

        def at(block, k):
            return buf.at[pl.ds(pl.multiple_of(block * features + k * size, size), size), :]

        def whole(block):
            return buf.at[pl.ds(pl.multiple_of(block * features, features), features), :]

        return Spread(stream_pieces, at, whole)

    def position_spreads(inner, edge):
        return (
            Spread(
                len(cuts), lambda block, k: inner.at[block, pl.ds(cuts[k][0], cuts[k][1]), :],
                lambda block: inner.at[block, pl.ds(EDGE, positions - 2 * EDGE), :],
            ),
            Spread(1, lambda block, k: edge.at[block], lambda block: edge.at[block], direct=True),
        )

    stream_copy = local_copy(stream, h_all.at[0, my_rows, :])
    barrier = pltpu.get_barrier_semaphore()
    for k in range(1, n_sp):
        pl.semaphore_signal(
            barrier, inc=1, device_id={"sp": lax.rem(s + k, n_sp), "tp": t}, device_id_type=MESH
        )
    for k in range(1, n_tp):
        pl.semaphore_signal(
            barrier, inc=1, device_id={"sp": s, "tp": lax.rem(t + k, n_tp)}, device_id_type=MESH
        )
    in_proj, out_proj = [], []
    out_parts = pieces_of(features, 128)
    for l in range(n_layers):
        in_proj.append(gathers(value_w, v_buf, l, [True], False) + gathers(gate_w, g_buf, l, [True], False))
        last = l + 1 == n_layers
        out_proj.append(gathers(out_w, o_buf, l, [last and i % 2 == 0 for i in range(out_parts)]))
    norm_rows[t] = norm_gain[...]
    out_rows[t] = out_gain[...]
    for l in range(n_layers):
        tap_rows[l, 0:n_taps, :] = taps[:, l, :].astype(F32)
    stream_copy.wait()
    pl.semaphore_wait(barrier, n_sp + n_tp - 2)

    spread = row_spread(h_all.at[0])
    cross = Cross(spread, x_all.at[0])
    for k in range(stream_pieces):
        spread.start_own(k)
        cross.forward(1, 0, k)
    early = max(1, out_parts // 2)
    for part in out_proj[0][:early]:
        part.send_x()
    for part in in_proj[0] + out_proj[0]:
        part.send_y()
    for l in range(1, n_layers):
        for part in in_proj[l]:
            part.send_y()
    gain_copies = exchange(norm_gain, norm_rows) + exchange(out_gain, out_rows)

    def turn_gain(i):
        rows = out_rows[i].astype(F32)
        fill = jnp.zeros((8 - n_layers, features), F32)
        out_cols[i * features : (i + 1) * features, :] = jnp.concatenate([rows, fill], axis=0).T

    def across_lanes(a, b):
        return lax.dot_general(a, b, (((1,), (1,)), ((), ())), preferred_element_type=F32)

    turned = [0]
    steps = [(k, j) for k in range(ny) for j in range(nx)]
    right, left = lax.rem(s + 1, n_sp), lax.rem(s + n_sp - 1, n_sp)
    has_right, has_left = s < n_sp - 1, s > 0

    def rows_at(q, count):
        return pl.ds(pl.multiple_of(q * count, count), count)

    for l in range(n_layers):
        last = l + 1 == n_layers
        groups_of_rows = [pl.ds(m * group, group) for m in range(groups)]
        if l == 0:
            waiting = list(out_proj[0][early:])
            for d in range(1, nz):
                for k in range(stream_pieces):
                    spread.step(d, k, cross.forward)
                    for way in ((1,) if d == 1 else (1, -1)):
                        cross.receive(way, d - 1, k)
                    if waiting and ((d - 1) * stream_pieces + k) % 2 == 1:
                        waiting.pop(0).send_x()
            for part in waiting:
                part.send_x()
            spread.wait_across()
            for d in range(1, nz):
                for way in (1, -1):
                    @pl.when(spread.has[way, d])
                    def _():
                        spread.wait_hand(way, d)
        for half, (part, buf) in enumerate(zip(in_proj[l], (v_buf, g_buf))):
            total = None
            for k in range(ny):
                part.arrive(k, 0)
                slot = slot_of(k, 0)
                one = jnp.dot(buf[l, slot], h_all[l, rows_at(slot, f_cols), :], preferred_element_type=F32)
                total = one if total is None else total + one
            acc[half] = total
        for k in range(stream_pieces):
            for way in (1, -1):
                cross.receive(way, nz - 1, k)
        cross.finish()
        if l > 0:
            for j in range(1, nx):
                factor_copies[j - 1].wait_recv()
                scale = peer_factor[l - 1, j - 1, 0:1, :]
                for k in range(ny):
                    here = pl.ds(k * f_cols, f_cols)
                    gain = out_cols[rows_at(k * nx + x, f_cols), l - 1 : l]
                    change = x_branch[l - 1, j - 1, here, :].astype(F32) * scale * gain
                    x_all[l, j - 1, here, :] = (x_all[l - 1, j - 1, here, :].astype(F32) + change).astype(BF16)
        part_copies = {}
        for m, rows in enumerate(groups_of_rows):
            for j in range(1, nx):
                for half, buf in enumerate((v_buf, g_buf)):
                    total = None
                    for k in range(ny):
                        block = rows_at(lax.rem(y + ny - k, ny), f_cols)
                        one = jnp.dot(
                            buf[l, slot_of(k, 0), rows, :], x_all[l, j - 1, block, :],
                            preferred_element_type=F32,
                        )
                        total = one if total is None else total + one
                    part_out[l, j - 1, half, rows, :] = total.astype(BF16)
                mine = part_out.at[l, j - 1, :, rows, :]
                send = send_slot()
                copy = remote(
                    mine, part_in.at[l, j - 1, :, rows, :], y * nx + lax.rem(x + nx - j, nx), t,
                    send, recv_slot(),
                )
                start(copy)
                leave(mine, send)
                part_copies[m, j] = copy

        edges = []
        for m, rows in enumerate(groups_of_rows):
            lanes = pl.ds(m * group, group)
            value, gate = acc[0, rows, :], acc[1, rows, :]
            for j in range(1, nx):
                part_copies[m, j].wait_recv()
                value = value + part_in[l, j - 1, 0, rows, :].astype(F32)
                gate = gate + part_in[l, j - 1, 1, rows, :].astype(F32)
            gated = (value * jax.nn.sigmoid(gate)).astype(BF16)
            wide[l, pl.ds(EDGE, positions), lanes] = gated.astype(F32).T
            pair = []
            for first, land, peer, here in (
                (positions, 0, right, has_right), (EDGE, EDGE + positions, left, has_left)
            ):
                mine, send = wide.at[l, pl.ds(first, EDGE), lanes], send_slot()
                copy = remote(mine, wide.at[l, pl.ds(land, EDGE), lanes], peer, t, send, recv_slot())
                start(copy, here)
                leave(mine, send, here)
                pair.append(copy)
            to_right, to_left = pair
            edges.append((to_right, to_left))

        for part in out_proj[l][:early] if l == 0 else out_proj[l]:
            part.flush()

        blank = jnp.zeros((EDGE, channels), F32)

        @pl.when(s == 0)
        def _():
            wide[l, 0:EDGE, :] = blank

        @pl.when(s == n_sp - 1)
        def _():
            wide[l, EDGE + positions : 2 * EDGE + positions, :] = blank

        def convolve(first, count, dst, land):
            while count:
                size = min(TILE, count)
                for m in range(groups):
                    lanes = pl.ds(m * group, group)
                    extent = size + 2 * EDGE
                    window = wide[l, pl.ds(first, extent), lanes]
                    total = None
                    for r in range(8):
                        moved = window if r == 0 else pltpu.roll(window, extent - r, 0)
                        for q in range(0, 2 * EDGE + 1, 8):
                            tap = q + r - (EDGE - reach)
                            if 0 <= tap < n_taps:
                                term = tap_rows[l, tap : tap + 1, lanes] * moved[q : q + size]
                                total = term if total is None else total + term
                    dst[l, t, pl.ds(land, size), lanes] = total.astype(BF16)
                first, land, count = first + size, land + size, count - size

        def total_up(phase, seen):
            square = seen.astype(F32) * seen.astype(F32)
            high = square.astype(BF16)
            low = (square - high.astype(F32)).astype(BF16)
            ones = jnp.ones((8, channels), BF16)
            sums[l, phase, t, 0:1, :] = across_lanes(ones, seen)[0:1]
            sums[l, phase, t, 1:2, :] = (across_lanes(ones, high) + across_lanes(ones, low))[0:1]
            return exchange(sums.at[l, phase, t], sums.at[l, phase])

        inner, edge = position_spreads(conv_all.at[l], conv_edge.at[l])
        border = jnp.zeros((EDGE, channels), BF16)
        conv_all[l, t, 0:EDGE, :] = border
        conv_all[l, t, positions - EDGE : positions, :] = border
        for k, (first, count) in enumerate(cuts):
            convolve(first, count, conv_all, first)
            inner.start_own(k)
        sum_copies = [total_up(0, conv_all[l, t]), None]

        def finish_edges():
            for to_right, to_left in edges:
                pl.when(has_left)(to_right.wait_recv)
                pl.when(has_right)(to_left.wait_recv)
            convolve(0, EDGE, conv_edge, 0)
            convolve(positions - EDGE, EDGE, conv_edge, EDGE)
            edge.start_own(0)
            conv_all[l, t, 0:EDGE, :] = conv_edge[l, t, 0:EDGE, :]
            conv_all[l, t, positions - EDGE : positions, :] = conv_edge[l, t, EDGE : 2 * EDGE, :]
            sum_copies[1] = total_up(1, conv_all[l, t])

        def settle(phase):
            arrived(sum_copies[phase])
            totals = jnp.sum(sums[l, phase], axis=0)
            average = totals[0:1] / width
            variance = totals[1:2] / width - average * average
            for i, row in enumerate((average, lax.rsqrt(variance + 1e-05))):
                column = jnp.broadcast_to(row, (LANES, positions)).T
                if channels > LANES:
                    column = jnp.concatenate([column] * (channels // LANES), axis=1)
                stat_cols[i] = column[:, :channels]

        def activate(src, block, first, count, land):
            gain = norm_rows[block].astype(F32)[l : l + 1]
            place = pl.ds(land, count)
            seen = src[l, block, pl.ds(first, count), :].astype(F32)
            scaled = (seen - stat_cols[0, place, :]) * stat_cols[1, place, :] * gain
            active[block, place, :] = (scaled / (1.0 + jnp.exp(-scaled))).astype(BF16)

        def activate_inner(block):
            activate(conv_all, block, EDGE, positions - 2 * EDGE, EDGE)

        def drain(spread, ready, consume, hook, finish=None, extra=None):
            def take(d):
                for way in (1, -1):
                    @pl.when(spread.has[way, d])
                    def _():
                        consume((z - way * d) * 2 + c)
                        spread.wait_hand(way, d)
                        consume((z - way * d) * 2 + 1 - c)

            when = min(2, nz - 1)
            for d in range(1, nz):
                for k in range(spread.pieces):
                    spread.step(d, k, extra)
                    hook((d - 1) * spread.pieces + k)
                if d == when:
                    ready()
                    consume(t)
                    spread.wait_across()
                    consume(z * 2 + 1 - c)
                if d >= when and d > 1:
                    take(d - 1)
            if finish is not None:
                finish()
            take(nz - 1)

        def conv_hook(i):
            if i == min(1, len(cuts) - 1):
                finish_edges()
            if l == 0:
                if i == 2:
                    arrived(gain_copies)
                if i >= 2 and turned[0] < n_tp:
                    turn_gain(turned[0])
                    turned[0] += 1
                if i % 3 == 1 and early + i // 3 < out_parts:
                    out_proj[l][early + i // 3].flush()
            if not last and i == 5:
                out_proj[l + 1][0].send_x()

        def catch_edges():
            for d in range(1, nz):
                edge.step(d, 0)

        drain(inner, lambda: settle(0), activate_inner, conv_hook, catch_edges)
        edge.wait_across()
        for d in range(1, nz):
            for way in (1, -1):
                @pl.when(edge.has[way, d])
                def _():
                    edge.wait_hand(way, d)
        settle(1)
        for block in range(n_tp):
            activate(conv_edge, block, 0, EDGE, 0)
            activate(conv_edge, block, EDGE, EDGE, positions - EDGE)
        while turned[0] < n_tp:
            turn_gain(turned[0])
            turned[0] += 1
        for part in out_proj[l]:
            part.flush()
        total = None
        for k, j in steps:
            slot = slot_of(k, j)
            for part in out_proj[l]:
                part.arrive(k, j)
            for i in range(c_cols // channels):
                one = across_lanes(
                    o_buf[l, slot, :, i * channels : (i + 1) * channels], active[slot * (c_cols // channels) + i]
                )
                total = one if total is None else total + one
        narrow_branch = total.astype(BF16)
        branch = narrow_branch.astype(F32)
        squares[l, t, 0:1, :] = jnp.sum(branch * branch, axis=0, keepdims=True)
        square_copies = exchange(squares.at[l, t], squares.at[l])

        def factor_of():
            arrived(square_copies)
            return lax.rsqrt(jnp.sum(squares[l], axis=0) / model + 1e-06)

        if last:
            factor = factor_of()
            gain = out_cols[my_rows, l : l + 1]
            fresh = h_all[l, my_rows, :].astype(F32) + branch * factor * gain
            result[...] = fresh.astype(BF16)
        else:
            branch_all[l, my_rows, :] = narrow_branch
            branch_spread = row_spread(branch_all.at[l])
            cross = Cross(branch_spread, x_branch.at[l])
            for k in range(stream_pieces):
                branch_spread.start_own(k)
                cross.forward(1, 0, k)
            for part in out_proj[l + 1]:
                part.send_y()

            factor, factor_copies = [None], []

            def scale_up():
                factor[0] = factor_of()
                own_factor[l, 0:1, :] = factor[0]
                for j in range(1, nx):
                    mine, send = own_factor.at[l], send_slot()
                    copy = remote(mine, peer_factor.at[l, j - 1], x_peer(j), t, send, recv_slot())
                    start(copy)
                    leave(mine, send)
                    factor_copies.append(copy)

            def renew(block):
                @pl.when((block == t) | (lax.rem(block // 2, nx) == x))
                def _():
                    rows = rows_at(block, features)
                    gain = out_cols[rows, l : l + 1]
                    change = branch_all[l, rows, :].astype(F32) * own_factor[l, 0:1, :] * gain
                    h_all[l + 1, rows, :] = (h_all[l, rows, :].astype(F32) + change).astype(BF16)

            def branch_hook(i):
                d, k = i // stream_pieces + 1, i % stream_pieces
                for way in ((1,) if d == 1 else (1, -1)):
                    cross.receive(way, d - 1, k)
                if i % 2 == 1 and 1 + i // 2 < out_parts:
                    out_proj[l + 1][1 + i // 2].send_x()

            drain(branch_spread, scale_up, renew, branch_hook, extra=cross.forward)

    for copy, condition in sent:
        if condition is None:
            copy.wait_send()
        else:
            pl.when(condition)(copy.wait_send)
    assert sends[0] == send_sem.shape[0], sends
    assert recvs[0] == recv_sem.shape[0], recvs
    assert local_count[0] == local_sem.shape[0], local_count


def slots_of(ny, nx, nz, layers, features, channels, positions):
    n_sp, far = ny * nx, 2 * (nz - 1)
    pieces, cuts, groups = pieces_of(features, 128), len(cuts_of(positions)), pieces_of(channels, LANES)
    small = 2 + 3 * layers + groups * (nx - 1) * layers + 2 * groups * layers + (layers - 1) * (nx - 1)
    send = layers * (3 * (1 + 2 * far) + (far + 1) * nx + 3) + small
    recv = layers * (3 + far * (pieces + 1 + cuts + 1 + 2) + (far + 1) * (pieces + 1) * (nx - 1)) + small
    recv += layers * (2 * (ny - 1) + (n_sp - 1) * pieces)
    local = 1 + layers * (2 + pieces)
    return send, recv, local


def on_device(n_sp, n_tp, stream, value_weight, gate_weight, conv_taps, norm_gain, out_weight, out_gain):
    layers, channels, f_cols = value_weight.shape
    features, positions = stream.shape
    c_cols = out_weight.shape[2]
    ny, nx = grid_of(n_sp)
    send, recv, local = slots_of(ny, nx, n_tp // 2, layers, features, channels, positions)
    vmem = pl.BlockSpec(memory_space=pltpu.VMEM)
    hbm = pl.BlockSpec(memory_space=pl.ANY)
    return pl.pallas_call(
        functools.partial(kernel, n_sp, n_tp, layers),
        out_shape=jax.ShapeDtypeStruct(stream.shape, BF16),
        in_specs=[hbm, hbm, hbm, vmem, vmem, hbm, vmem],
        out_specs=vmem,
        scratch_shapes=[
            pltpu.VMEM((layers, n_tp * features, positions), BF16),
            pltpu.VMEM((layers, nx - 1, n_tp * features // nx, positions), BF16),
            pltpu.VMEM((max(layers - 1, 1), nx - 1, n_tp * features // nx, positions), BF16),
            pltpu.VMEM((layers, 1, positions), F32),
            pltpu.VMEM((layers, nx - 1, 1, positions), F32),
            pltpu.VMEM((layers, n_tp, positions, channels), BF16),
            pltpu.VMEM((layers, n_tp, 2 * EDGE, channels), BF16),
            pltpu.VMEM((max(layers - 1, 1), n_tp * features, positions), BF16),
            pltpu.VMEM((n_tp, positions, channels), BF16),
            pltpu.VMEM((layers, n_sp, channels, f_cols), BF16),
            pltpu.VMEM((layers, n_sp, channels, f_cols), BF16),
            pltpu.VMEM((layers, n_sp, features, c_cols), BF16),
            pltpu.VMEM((layers, nx - 1, 2, channels, positions), BF16),
            pltpu.VMEM((layers, nx - 1, 2, channels, positions), BF16),
            pltpu.VMEM((layers, positions + 2 * EDGE, channels), F32),
            pltpu.VMEM((2, positions, channels), F32),
            pltpu.VMEM((layers, 2 * EDGE, channels), F32),
            pltpu.VMEM((2, channels, positions), F32),
            pltpu.VMEM((layers, 2, n_tp, 2, positions), F32),
            pltpu.VMEM((layers, n_tp, 1, positions), F32),
            pltpu.VMEM((n_tp, layers, channels), BF16),
            pltpu.VMEM((n_tp, layers, features), BF16),
            pltpu.VMEM((n_tp * features, 8), F32),
            pltpu.SemaphoreType.DMA((local,)),
            pltpu.SemaphoreType.DMA((send,)),
            pltpu.SemaphoreType.DMA((recv,)),
        ],
        compiler_params=pltpu.CompilerParams(
            collective_id=0, has_side_effects=True, vmem_limit_bytes=60 * 1024 * 1024
        ),
    )(stream, value_weight, gate_weight, jnp.transpose(conv_taps, (2, 0, 1)), norm_gain, out_weight, out_gain)


def solution(mesh):
    return jax.shard_map(
        functools.partial(on_device, mesh.shape["sp"], mesh.shape["tp"]),
        mesh=mesh,
        in_specs=(
            P("tp", "sp"),
            P(None, "tp", "sp"),
            P(None, "tp", "sp"),
            P(None, "tp", None),
            P(None, "tp"),
            P(None, "tp", "sp"),
            P(None, "tp"),
        ),
        out_specs=P("tp", "sp"),
        check_vma=False,
    )
```

```python
import functools

import jax
import jax.numpy as jnp
from jax import lax
from jax.experimental import pallas as pl
from jax.experimental.pallas import tpu as pltpu
from jax.sharding import PartitionSpec as P

MESH = pl.DeviceIdType.MESH
F32 = jnp.float32
BF16 = jnp.bfloat16
LANES = 128
EDGE = 16
TILE = 64


def grid_of(count):
    nx = int(count**0.5)
    while count % nx:
        nx -= 1
    return count // nx, nx


def pieces_of(rows, size):
    return max(1, rows // size)


def cuts_of(positions):
    inner = positions - 2 * EDGE
    count = max(1, inner // 64)
    size = inner // count // EDGE * EDGE
    cuts = [(EDGE + k * size, size) for k in range(count - 1)]
    first = EDGE + (count - 1) * size
    cuts.append((first, positions - EDGE - first))
    return cuts


def kernel(
    n_sp, n_tp, n_layers,
    stream, value_w, gate_w, taps, norm_gain, out_w, out_gain,
    result,
    h_all, x_all, x_branch, own_factor, peer_factor, conv_all, conv_edge, branch_all, active, v_buf, g_buf, o_buf, part_out, part_in, wide, stat_cols, tap_rows,
    acc, sums, squares, norm_rows, out_rows, out_cols,
    local_sem, send_sem, recv_sem,
):
    ny, nx = grid_of(n_sp)
    nz = n_tp // 2
    s, t = lax.axis_index("sp"), lax.axis_index("tp")
    y, x = s // nx, s % nx
    z, c = t // 2, t % 2
    features, positions = stream.shape
    channels = value_w.shape[1]
    f_cols = value_w.shape[2]
    c_cols = out_w.shape[2]
    width = channels * n_tp
    model = features * n_tp
    n_taps = taps.shape[0]
    reach = n_taps // 2
    groups = pieces_of(channels, LANES)
    group = channels // groups
    sends, recvs, sent = [0], [0], []

    def send_slot():
        sends[0] += 1
        return sends[0] - 1

    def recv_slot(count=1):
        recvs[0] += count
        return recvs[0] - count

    def remote(src, dst, sp, tp, send=None, recv=None):
        return pltpu.make_async_remote_copy(
            src_ref=src, dst_ref=dst,
            send_sem=send_sem.at[0 if send is None else send], recv_sem=recv_sem.at[0 if recv is None else recv],
            device_id={"sp": sp, "tp": tp}, device_id_type=MESH,
        )

    def start(copy, condition=None):
        if condition is None:
            copy.start()
        else:
            pl.when(condition)(copy.start)

    tag, banks = [None], {}

    def leave(ref, send, condition=None):
        sent.append((remote(ref, ref, s, t, send=send), condition, tag[0]))

    def finish_sends(name=None):
        chosen = [entry for entry in sent if name is None or entry[2] == name]
        sent[:] = [entry for entry in sent if name is not None and entry[2] != name]
        for entry in chosen:
            if entry[1] is None:
                entry[0].wait_send()
            else:
                pl.when(entry[1])(entry[0].wait_send)

    def banked(name, make):
        here, tag[0] = (sends[0], recvs[0]), name
        again = name in banks
        if again:
            assert not [entry for entry in sent if entry[2] == name]
            sends[0], recvs[0] = banks[name]
        banks.setdefault(name, here)
        made = make()
        if again:
            sends[0], recvs[0] = here
        tag[0] = None
        return made

    def slot_of(k, j):
        return lax.rem(y + ny - k, ny) * nx + lax.rem(x + nx - j, nx)

    def x_peer(j):
        return y * nx + lax.rem(x + j, nx)

    def y_peer(k):
        return lax.rem(y + k, ny) * nx + x

    local_count = [0]

    def local_copy(src, dst):
        i = local_count[0]
        local_count[0] += 1
        copy = pltpu.make_async_copy(src, dst, local_sem.at[i])
        copy.start()
        return copy

    class Gather:
        def __init__(self, src, dst, x_first, whole, send):
            self.copies, self.own_x, self.own_y, self.relays = {}, [], [], []
            for k in range(ny):
                for j in range(nx if whole else 1):
                    if k == 0 and j == 0:
                        continue
                    if x_first:
                        along_x = k == 0
                        origin = (0, 0) if along_x else (0, j)
                    else:
                        along_x = j > 0
                        origin = (k, 0) if along_x else (0, 0)
                    own = origin == (0, 0)
                    target = x_peer(j) if along_x else y_peer(k)
                    origin_slot = slot_of(*origin)
                    copy = remote(
                        src if own else dst(origin_slot), dst(origin_slot), target, t, send=send, recv=recv_slot()
                    )
                    self.copies[k, j] = copy
                    if not own:
                        self.relays.append((copy, origin))
                    elif along_x:
                        self.own_x.append(copy)
                    else:
                        self.own_y.append(copy)
            self.local = local_copy(src, dst(s))
            self.here, self.done = set(), set()

        def once(self, name):
            fresh = name not in self.done
            self.done.add(name)
            return fresh

        def send_x(self):
            if self.once("x"):
                for copy in self.own_x:
                    start(copy)

        def send_y(self):
            if self.once("y"):
                for copy in self.own_y:
                    start(copy)

        def relay(self):
            if self.once("relay"):
                for copy, origin in self.relays:
                    self.arrive(*origin)
                    start(copy)

        def flush(self):
            self.send_x()
            self.send_y()
            self.relay()

        def arrive(self, k, j):
            if (k, j) not in self.here:
                self.here.add((k, j))
                if k == 0 and j == 0:
                    self.local.wait()
                else:
                    self.copies[k, j].wait_recv()

    def gathers(w_ref, buf, l, orders, whole=True):
        rows = w_ref.shape[1] // len(orders)
        made, send = [], send_slot()
        leave(buf.at[l, pl.ds(0, (n_sp if whole else ny) - 1)], send)
        for i, x_first in enumerate(orders):
            part = pl.ds(i * rows, rows)
            made.append(Gather(w_ref.at[l, part], lambda q, part=part: buf.at[l, q, part], x_first, whole, send))
        return made

    class Spread:
        def __init__(self, pieces, at, whole, direct=False):
            def place(zz, cc, k):
                return at(jnp.clip(zz, 0, nz - 1) * 2 + cc, k)

            def full(zz, cc):
                return whole(jnp.clip(zz, 0, nz - 1) * 2 + cc)

            other = z * 2 + 1 - c
            self.pieces, self.place, self.direct = pieces, place, direct
            send, recv = send_slot(), recv_slot()
            self.across = [
                remote(place(z, c, k), place(z, c, k), s, other, send, recv) for k in range(pieces)
            ]
            self.landed = remote(full(z, 1 - c), full(z, 1 - c), s, other, recv=recv)
            leave(full(z, c), send)
            self.along, self.goes, self.hand, self.has, self.handed = {}, {}, {}, {}, {}
            for d in range(1, nz):
                for way in (1, -1):
                    has = (z - way * d >= 0) & (z - way * d < nz)
                    self.has[way, d] = has
                    send, hand_send, hand_recv = send_slot(), send_slot(), recv_slot()
                    if direct:
                        from_z, to_z = z, z + way * d
                        self.goes[way, d] = (to_z >= 0) & (to_z < nz)
                    else:
                        from_z, to_z = z - way * (d - 1), z + way
                        self.goes[way, d] = (from_z >= 0) & (from_z < nz) & (to_z >= 0) & (to_z < nz)
                    target = jnp.clip(to_z, 0, nz - 1) * 2 + c
                    for k in range(pieces):
                        held = place(from_z, c, k)
                        self.along[way, d, k] = remote(held, held, s, target, send, recv_slot())
                        seen = place(z - way * d, c, k)
                        self.hand[way, d, k] = remote(seen, seen, s, other, hand_send, hand_recv)
                    block = full(z - way * d, c)
                    self.handed[way, d] = remote(block, block, s, other, recv=hand_recv)
                    leave(block, send, self.goes[way, d])
                    leave(block, hand_send, has)

        def send(self, way, d, k):
            start(self.along[way, d, k], self.goes[way, d])

        def start_own(self, k):
            for d in range(1, nz) if self.direct else (1,):
                for way in (1, -1):
                    self.send(way, d, k)
            start(self.across[k])

        def step(self, d, k, extra=None):
            for way in (1, -1):
                pl.when(self.has[way, d])(self.along[way, d, k].wait_recv)
                if d + 1 < nz and not self.direct:
                    self.send(way, d + 1, k)
                start(self.hand[way, d, k], self.has[way, d])
                if extra is not None:
                    extra(way, d, k)

        def wait_across(self):
            self.landed.wait_recv()

        def wait_hand(self, way, d):
            self.handed[way, d].wait_recv()

    def ways_at(d):
        return (1, -1) if d else (1,)

    class Cross:
        def __init__(self, spread, land):
            self.spread, self.land = spread, land
            self.size = features // spread.pieces
            self.sends, self.base, self.hands = {}, {}, {}
            for d in range(nz):
                for way in ways_at(d):
                    ok, q, owner = self.facts(way, d)
                    block = self.rows(q, 0, spread.pieces)
                    self.sends[way, d] = send_slot()
                    leave(land.at[0, block, :], self.sends[way, d], ok & (owner != x))
                    for k in range(spread.pieces):
                        self.base[way, d, k] = recv_slot(nx - 1)
                    for j in range(1, nx):
                        send, recv = send_slot(), recv_slot()
                        place = land.at[j - 1, block, :]
                        mine = ok & (owner == x)
                        self.hands[way, d, j] = (send, recv, remote(place, place, s, t, recv=recv), mine)
                        leave(place, send, mine)

        def facts(self, way, d):
            zz = z - way * d
            ok = (zz >= 0) & (zz < nz)
            q = jnp.clip(zz, 0, nz - 1)
            return ok, q, lax.rem(q, nx)

        def rows(self, q, k, count=1):
            size = self.size
            row = (q // nx * 2 + c) * features + k * size
            return pl.ds(pl.multiple_of(row, size), size * count)

        def forward(self, way, d, k):
            ok, q, owner = self.facts(way, d)
            pick = jnp.clip(lax.rem(owner - x + nx, nx) - 1, 0, nx - 2)
            copy = remote(
                self.spread.place(q, c, k), self.land.at[pick, self.rows(q, k), :], y * nx + owner, t,
                self.sends[way, d], self.base[way, d, k] + pick,
            )
            start(copy, ok & (owner != x))

        def receive(self, way, d, k):
            _, q, _ = self.facts(way, d)
            for j in range(1, nx):
                send, recv, _, mine = self.hands[way, d, j]
                here = self.land.at[j - 1, self.rows(q, k), :]
                landed = remote(here, here, s, t, recv=self.base[way, d, k] + j - 1)
                hand = remote(here, here, s, z * 2 + 1 - c, send, recv)

                @pl.when(mine)
                def _():
                    landed.wait_recv()
                    hand.start()

        def receive_all(self, d):
            for k in range(self.spread.pieces):
                for way in ways_at(d):
                    self.receive(way, d, k)

        def finish(self):
            for _, _, handed, mine in self.hands.values():
                pl.when(mine)(handed.wait_recv)

    def exchange(src, buf):
        send, recv = send_slot(), recv_slot()
        others = buf.at[pl.ds(0, n_tp - 1)]
        for k in range(1, n_tp):
            start(remote(src, buf.at[t], s, lax.rem(t + k, n_tp), send, recv))
        leave(others, send)
        return [remote(others, others, s, t, recv=recv)]

    def arrived(copies):
        for copy in copies:
            copy.wait_recv()

    my_rows = pl.ds(pl.multiple_of(t * features, features), features)
    stream_pieces = pieces_of(features, 128)
    cuts = cuts_of(positions)

    def row_spread(buf):
        size = features // stream_pieces

        def at(block, k):
            return buf.at[pl.ds(pl.multiple_of(block * features + k * size, size), size), :]

        def whole(block):
            return buf.at[pl.ds(pl.multiple_of(block * features, features), features), :]

        return Spread(stream_pieces, at, whole)

    def position_spreads(inner, edge):
        return (
            Spread(
                len(cuts), lambda block, k: inner.at[block, pl.ds(cuts[k][0], cuts[k][1]), :],
                lambda block: inner.at[block, pl.ds(EDGE, positions - 2 * EDGE), :],
            ),
            Spread(1, lambda block, k: edge.at[block], lambda block: edge.at[block], direct=True),
        )

    stream_copy = local_copy(stream, h_all.at[0, my_rows, :])
    barrier = pltpu.get_barrier_semaphore()
    above, below = z + 1 < nz, z > 0
    near = [(x_peer(j), t, None) for j in range(1, nx)] + [(y_peer(k), t, None) for k in range(1, ny)]
    near += [(s, z * 2 + 1 - c, None), (s, (z + 1) * 2 + c, above), (s, (z - 1) * 2 + c, below)]
    for sp, tp, here in near:
        def greet(sp=sp, tp=tp):
            pl.semaphore_signal(barrier, inc=1, device_id={"sp": sp, "tp": tp}, device_id_type=MESH)

        if here is None:
            greet()
        else:
            pl.when(here)(greet)
    in_proj, out_proj = [], []
    out_parts = pieces_of(features, 128)
    for l in range(n_layers):
        in_proj.append(gathers(value_w, v_buf, l, [True], False) + gathers(gate_w, g_buf, l, [True], False))
        last = l + 1 == n_layers
        out_proj.append(gathers(out_w, o_buf, l, [last and i % 2 == 0 for i in range(out_parts)]))
    norm_rows[t] = norm_gain[...]
    out_rows[t] = out_gain[...]
    for l in range(n_layers):
        tap_rows[l, 0:n_taps, :] = taps[:, l, :].astype(F32)
    stream_copy.wait()
    @pl.when(above & below)
    def _():
        pl.semaphore_wait(barrier, nx + ny + 1)

    @pl.when(jnp.logical_not(above & below))
    def _():
        pl.semaphore_wait(barrier, nx + ny)

    spread = banked("rows", lambda: row_spread(h_all.at[0]))
    cross = banked("cross", lambda: Cross(spread, x_all.at[0]))
    for k in range(stream_pieces):
        spread.start_own(k)
        cross.forward(1, 0, k)
    early = max(1, out_parts // 2)
    for part in out_proj[0][:early]:
        part.send_x()
    for part in in_proj[0] + out_proj[0]:
        part.send_y()
    for l in range(1, n_layers):
        for part in in_proj[l]:
            part.send_y()

    def turn_gain(i):
        rows = out_rows[i].astype(F32)
        fill = jnp.zeros((8 - n_layers, features), F32)
        out_cols[i * features : (i + 1) * features, :] = jnp.concatenate([rows, fill], axis=0).T

    def across_lanes(a, b):
        return lax.dot_general(a, b, (((1,), (1,)), ((), ())), preferred_element_type=F32)

    turned = [0]
    steps = [(k, j) for k in range(ny) for j in range(nx)]
    right, left = lax.rem(s + 1, n_sp), lax.rem(s + n_sp - 1, n_sp)
    has_right, has_left = s < n_sp - 1, s > 0

    def rows_at(q, count):
        return pl.ds(pl.multiple_of(q * count, count), count)

    for l in range(n_layers):
        last = l + 1 == n_layers
        groups_of_rows = [pl.ds(m * group, group) for m in range(groups)]
        if l == 0:
            waiting = list(out_proj[0][early:])
            for d in range(1, nz):
                for k in range(stream_pieces):
                    spread.step(d, k, cross.forward)
                    for way in ways_at(d - 2) if d > 1 else ():
                        cross.receive(way, d - 2, k)
                    if waiting and ((d - 1) * stream_pieces + k) % 2 == 1:
                        waiting.pop(0).send_x()
            for part in waiting:
                part.send_x()
            spread.wait_across()
            for d in range(1, nz):
                for way in (1, -1):
                    @pl.when(spread.has[way, d])
                    def _():
                        spread.wait_hand(way, d)
            gain_copies = exchange(norm_gain, norm_rows) + exchange(out_gain, out_rows)
        if nz > 1:
            cross.receive_all(nz - 2)
        for half, (part, buf) in enumerate(zip(in_proj[l], (v_buf, g_buf))):
            total = None
            for k in range(ny):
                part.arrive(k, 0)
                slot = slot_of(k, 0)
                one = jnp.dot(buf[l, slot], h_all[l, rows_at(slot, f_cols), :], preferred_element_type=F32)
                total = one if total is None else total + one
            acc[half] = total
        cross.receive_all(nz - 1)
        cross.finish()
        if l > 0:
            for j in range(1, nx):
                factor_copies[j - 1].wait_recv()
                scale = peer_factor[l - 1, j - 1, 0:1, :]
                for k in range(ny):
                    here = pl.ds(k * f_cols, f_cols)
                    gain = out_cols[rows_at(k * nx + x, f_cols), l - 1 : l]
                    change = x_branch[l - 1, j - 1, here, :].astype(F32) * scale * gain
                    x_all[l, j - 1, here, :] = (x_all[l - 1, j - 1, here, :].astype(F32) + change).astype(BF16)
        part_copies = {}
        for m, rows in enumerate(groups_of_rows):
            for j in range(1, nx):
                for half, buf in enumerate((v_buf, g_buf)):
                    total = None
                    for k in range(ny):
                        block = rows_at(lax.rem(y + ny - k, ny), f_cols)
                        one = jnp.dot(
                            buf[l, slot_of(k, 0), rows, :], x_all[l, j - 1, block, :],
                            preferred_element_type=F32,
                        )
                        total = one if total is None else total + one
                    part_out[l, j - 1, half, rows, :] = total.astype(BF16)
                mine = part_out.at[l, j - 1, :, rows, :]
                send = send_slot()
                copy = remote(
                    mine, part_in.at[l, j - 1, :, rows, :], y * nx + lax.rem(x + nx - j, nx), t,
                    send, recv_slot(),
                )
                start(copy)
                leave(mine, send)
                part_copies[m, j] = copy

        edges = []
        for m, rows in enumerate(groups_of_rows):
            lanes = pl.ds(m * group, group)
            value, gate = acc[0, rows, :], acc[1, rows, :]
            for j in range(1, nx):
                part_copies[m, j].wait_recv()
                value = value + part_in[l, j - 1, 0, rows, :].astype(F32)
                gate = gate + part_in[l, j - 1, 1, rows, :].astype(F32)
            gated = (value * jax.nn.sigmoid(gate)).astype(BF16)
            wide[l, pl.ds(EDGE, positions), lanes] = gated.astype(F32).T
            pair = []
            for first, land, peer, here in (
                (positions, 0, right, has_right), (EDGE, EDGE + positions, left, has_left)
            ):
                mine, send = wide.at[l, pl.ds(first, EDGE), lanes], send_slot()
                copy = remote(mine, wide.at[l, pl.ds(land, EDGE), lanes], peer, t, send, recv_slot())
                start(copy, here)
                leave(mine, send, here)
                pair.append(copy)
            to_right, to_left = pair
            edges.append((to_right, to_left))

        for part in out_proj[l][:early] if l == 0 else out_proj[l]:
            part.flush()

        blank = jnp.zeros((EDGE, channels), F32)

        @pl.when(s == 0)
        def _():
            wide[l, 0:EDGE, :] = blank

        @pl.when(s == n_sp - 1)
        def _():
            wide[l, EDGE + positions : 2 * EDGE + positions, :] = blank

        def convolve(first, count, dst, land):
            while count:
                size = min(TILE, count)
                for m in range(groups):
                    lanes = pl.ds(m * group, group)
                    extent = size + 2 * EDGE
                    window = wide[l, pl.ds(first, extent), lanes]
                    total = None
                    for r in range(8):
                        moved = window if r == 0 else pltpu.roll(window, extent - r, 0)
                        for q in range(0, 2 * EDGE + 1, 8):
                            tap = q + r - (EDGE - reach)
                            if 0 <= tap < n_taps:
                                term = tap_rows[l, tap : tap + 1, lanes] * moved[q : q + size]
                                total = term if total is None else total + term
                    dst[l, t, pl.ds(land, size), lanes] = total.astype(BF16)
                first, land, count = first + size, land + size, count - size

        def total_up(phase, seen):
            square = seen.astype(F32) * seen.astype(F32)
            high = square.astype(BF16)
            low = (square - high.astype(F32)).astype(BF16)
            ones = jnp.ones((8, channels), BF16)
            sums[l, phase, t, 0:1, :] = across_lanes(ones, seen)[0:1]
            sums[l, phase, t, 1:2, :] = (across_lanes(ones, high) + across_lanes(ones, low))[0:1]
            return exchange(sums.at[l, phase, t], sums.at[l, phase])

        inner, edge = banked("conv", lambda: position_spreads(conv_all.at[l], conv_edge.at[l]))
        border = jnp.zeros((EDGE, channels), BF16)
        conv_all[l, t, 0:EDGE, :] = border
        conv_all[l, t, positions - EDGE : positions, :] = border
        for k, (first, count) in enumerate(cuts):
            convolve(first, count, conv_all, first)
            inner.start_own(k)
        sum_copies = [total_up(0, conv_all[l, t]), None]

        def finish_edges():
            for to_right, to_left in edges:
                pl.when(has_left)(to_right.wait_recv)
                pl.when(has_right)(to_left.wait_recv)
            convolve(0, EDGE, conv_edge, 0)
            convolve(positions - EDGE, EDGE, conv_edge, EDGE)
            edge.start_own(0)
            conv_all[l, t, 0:EDGE, :] = conv_edge[l, t, 0:EDGE, :]
            conv_all[l, t, positions - EDGE : positions, :] = conv_edge[l, t, EDGE : 2 * EDGE, :]
            sum_copies[1] = total_up(1, conv_all[l, t])

        def settle(phase):
            arrived(sum_copies[phase])
            totals = jnp.sum(sums[l, phase], axis=0)
            average = totals[0:1] / width
            variance = totals[1:2] / width - average * average
            for i, row in enumerate((average, lax.rsqrt(variance + 1e-05))):
                column = jnp.broadcast_to(row, (LANES, positions)).T
                if channels > LANES:
                    column = jnp.concatenate([column] * (channels // LANES), axis=1)
                stat_cols[i] = column[:, :channels]

        def activate(src, block, first, count, land):
            gain = norm_rows[block].astype(F32)[l : l + 1]
            place = pl.ds(land, count)
            seen = src[l, block, pl.ds(first, count), :].astype(F32)
            scaled = (seen - stat_cols[0, place, :]) * stat_cols[1, place, :] * gain
            active[block, place, :] = (scaled / (1.0 + jnp.exp(-scaled))).astype(BF16)

        def activate_inner(block):
            activate(conv_all, block, EDGE, positions - 2 * EDGE, EDGE)

        def drain(spread, ready, consume, hook, finish=None, extra=None):
            def take(d):
                for way in (1, -1):
                    @pl.when(spread.has[way, d])
                    def _():
                        consume((z - way * d) * 2 + c)
                        spread.wait_hand(way, d)
                        consume((z - way * d) * 2 + 1 - c)

            when = min(2, nz - 1)
            for d in range(1, nz):
                for k in range(spread.pieces):
                    spread.step(d, k, extra)
                    hook((d - 1) * spread.pieces + k)
                if d == when:
                    ready()
                    consume(t)
                    spread.wait_across()
                    consume(z * 2 + 1 - c)
                if d >= when and d > 1:
                    take(d - 1)
            if finish is not None:
                finish()
            take(nz - 1)

        def conv_hook(i):
            if i == min(1, len(cuts) - 1):
                finish_edges()
            if l == 0:
                if i == 2:
                    arrived(gain_copies)
                    finish_sends("rows")
                    finish_sends("cross")
                if i >= 2 and turned[0] < n_tp:
                    turn_gain(turned[0])
                    turned[0] += 1
                if i % 3 == 1 and early + i // 3 < out_parts:
                    out_proj[l][early + i // 3].flush()
            if not last and i in (3, 5):
                for part in out_proj[l + 1][: i // 2]:
                    part.send_x()

        def catch_edges():
            for d in range(1, nz):
                edge.step(d, 0)

        drain(inner, lambda: settle(0), activate_inner, conv_hook, catch_edges)
        edge.wait_across()
        for d in range(1, nz):
            for way in (1, -1):
                @pl.when(edge.has[way, d])
                def _():
                    edge.wait_hand(way, d)
        settle(1)
        for block in range(n_tp):
            activate(conv_edge, block, 0, EDGE, 0)
            activate(conv_edge, block, EDGE, EDGE, positions - EDGE)
        while turned[0] < n_tp:
            turn_gain(turned[0])
            turned[0] += 1
        for part in out_proj[l]:
            part.flush()
        total = None
        for k, j in steps:
            slot = slot_of(k, j)
            for part in out_proj[l]:
                part.arrive(k, j)
            for i in range(c_cols // channels):
                one = across_lanes(
                    o_buf[l, slot, :, i * channels : (i + 1) * channels], active[slot * (c_cols // channels) + i]
                )
                total = one if total is None else total + one
        narrow_branch = total.astype(BF16)
        branch = narrow_branch.astype(F32)
        squares[l, t, 0:1, :] = jnp.sum(branch * branch, axis=0, keepdims=True)
        square_copies = exchange(squares.at[l, t], squares.at[l])

        def factor_of():
            arrived(square_copies)
            return lax.rsqrt(jnp.sum(squares[l], axis=0) / model + 1e-06)

        if last:
            factor = factor_of()
            gain = out_cols[my_rows, l : l + 1]
            fresh = h_all[l, my_rows, :].astype(F32) + branch * factor * gain
            result[...] = fresh.astype(BF16)
        else:
            branch_all[l, my_rows, :] = narrow_branch
            branch_spread = banked("rows", lambda: row_spread(branch_all.at[l]))
            cross = banked("cross", lambda: Cross(branch_spread, x_branch.at[l]))
            for k in range(stream_pieces):
                branch_spread.start_own(k)
                cross.forward(1, 0, k)
            for part in out_proj[l + 1]:
                part.send_y()

            factor, factor_copies = [None], []

            def scale_up():
                factor[0] = factor_of()
                own_factor[l, 0:1, :] = factor[0]
                for j in range(1, nx):
                    mine, send = own_factor.at[l], send_slot()
                    copy = remote(mine, peer_factor.at[l, j - 1], x_peer(j), t, send, recv_slot())
                    start(copy)
                    leave(mine, send)
                    factor_copies.append(copy)

            def renew(block):
                @pl.when((block == t) | (lax.rem(block // 2, nx) == x))
                def _():
                    rows = rows_at(block, features)
                    gain = out_cols[rows, l : l + 1]
                    change = branch_all[l, rows, :].astype(F32) * own_factor[l, 0:1, :] * gain
                    h_all[l + 1, rows, :] = (h_all[l, rows, :].astype(F32) + change).astype(BF16)

            def branch_hook(i):
                d, k = i // stream_pieces + 1, i % stream_pieces
                for way in ways_at(d - 2) if d > 1 else ():
                    cross.receive(way, d - 2, k)
                if i == 2:
                    finish_sends("conv")
                if i % 2 == 1 and 1 + i // 2 < out_parts:
                    out_proj[l + 1][1 + i // 2].send_x()

            drain(branch_spread, scale_up, renew, branch_hook, extra=cross.forward)

    finish_sends()
    assert sends[0] == send_sem.shape[0], sends
    assert recvs[0] == recv_sem.shape[0], recvs
    assert local_count[0] == local_sem.shape[0], local_count


def slots_of(ny, nx, nz, layers, features, channels, positions):
    n_sp, far = ny * nx, 2 * (nz - 1)
    pieces, cuts, groups = pieces_of(features, 128), len(cuts_of(positions)), pieces_of(channels, LANES)
    small = 2 + 3 * layers + groups * (nx - 1) * layers + 2 * groups * layers + (layers - 1) * (nx - 1)
    send = 3 * (1 + 2 * far) + (far + 1) * nx + 3 * layers + small
    recv = 3 + far * (pieces + 1 + cuts + 1 + 2) + (far + 1) * (pieces + 1) * (nx - 1) + small
    recv += layers * (2 * (ny - 1) + (n_sp - 1) * pieces)
    local = 1 + layers * (2 + pieces)
    return send, recv, local


def on_device(n_sp, n_tp, stream, value_weight, gate_weight, conv_taps, norm_gain, out_weight, out_gain):
    layers, channels, f_cols = value_weight.shape
    features, positions = stream.shape
    c_cols = out_weight.shape[2]
    ny, nx = grid_of(n_sp)
    send, recv, local = slots_of(ny, nx, n_tp // 2, layers, features, channels, positions)
    vmem = pl.BlockSpec(memory_space=pltpu.VMEM)
    hbm = pl.BlockSpec(memory_space=pl.ANY)
    return pl.pallas_call(
        functools.partial(kernel, n_sp, n_tp, layers),
        out_shape=jax.ShapeDtypeStruct(stream.shape, BF16),
        in_specs=[hbm, hbm, hbm, vmem, vmem, hbm, vmem],
        out_specs=vmem,
        scratch_shapes=[
            pltpu.VMEM((layers, n_tp * features, positions), BF16),
            pltpu.VMEM((layers, nx - 1, n_tp * features // nx, positions), BF16),
            pltpu.VMEM((max(layers - 1, 1), nx - 1, n_tp * features // nx, positions), BF16),
            pltpu.VMEM((layers, 1, positions), F32),
            pltpu.VMEM((layers, nx - 1, 1, positions), F32),
            pltpu.VMEM((layers, n_tp, positions, channels), BF16),
            pltpu.VMEM((layers, n_tp, 2 * EDGE, channels), BF16),
            pltpu.VMEM((max(layers - 1, 1), n_tp * features, positions), BF16),
            pltpu.VMEM((n_tp, positions, channels), BF16),
            pltpu.VMEM((layers, n_sp, channels, f_cols), BF16),
            pltpu.VMEM((layers, n_sp, channels, f_cols), BF16),
            pltpu.VMEM((layers, n_sp, features, c_cols), BF16),
            pltpu.VMEM((layers, nx - 1, 2, channels, positions), BF16),
            pltpu.VMEM((layers, nx - 1, 2, channels, positions), BF16),
            pltpu.VMEM((layers, positions + 2 * EDGE, channels), F32),
            pltpu.VMEM((2, positions, channels), F32),
            pltpu.VMEM((layers, 2 * EDGE, channels), F32),
            pltpu.VMEM((2, channels, positions), F32),
            pltpu.VMEM((layers, 2, n_tp, 2, positions), F32),
            pltpu.VMEM((layers, n_tp, 1, positions), F32),
            pltpu.VMEM((n_tp, layers, channels), BF16),
            pltpu.VMEM((n_tp, layers, features), BF16),
            pltpu.VMEM((n_tp * features, 8), F32),
            pltpu.SemaphoreType.DMA((local,)),
            pltpu.SemaphoreType.DMA((send,)),
            pltpu.SemaphoreType.DMA((recv,)),
        ],
        compiler_params=pltpu.CompilerParams(
            collective_id=0, has_side_effects=True, vmem_limit_bytes=60 * 1024 * 1024
        ),
    )(stream, value_weight, gate_weight, jnp.transpose(conv_taps, (2, 0, 1)), norm_gain, out_weight, out_gain)


def solution(mesh):
    return jax.shard_map(
        functools.partial(on_device, mesh.shape["sp"], mesh.shape["tp"]),
        mesh=mesh,
        in_specs=(
            P("tp", "sp"),
            P(None, "tp", "sp"),
            P(None, "tp", "sp"),
            P(None, "tp", None),
            P(None, "tp"),
            P(None, "tp", "sp"),
            P(None, "tp"),
        ),
        out_specs=P("tp", "sp"),
        check_vma=False,
    )
```

```python
import functools

import jax
import jax.numpy as jnp
from jax import lax
from jax.experimental import pallas as pl
from jax.experimental.pallas import tpu as pltpu
from jax.sharding import PartitionSpec as P

MESH = pl.DeviceIdType.MESH
F32 = jnp.float32
BF16 = jnp.bfloat16
LANES = 128
EDGE = 16
TILE = 64


def grid_of(count):
    nx = int(count**0.5)
    while count % nx:
        nx -= 1
    return count // nx, nx


def pieces_of(rows, size):
    return max(1, rows // size)


def cuts_of(positions):
    inner = positions - 2 * EDGE
    count = max(1, inner // 64)
    size = inner // count // EDGE * EDGE
    cuts = [(EDGE + k * size, size) for k in range(count - 1)]
    first = EDGE + (count - 1) * size
    cuts.append((first, positions - EDGE - first))
    return cuts


def kernel(
    n_sp, n_tp, n_layers,
    stream, value_w, gate_w, taps, norm_gain, out_w, out_gain,
    result,
    h_all, x_all, x_branch, own_factor, peer_factor, conv_all, conv_edge, branch_all, active, v_buf, g_buf, o_buf, part_out, part_in, wide, stat_cols, tap_rows,
    acc, sums, squares, norm_rows, out_rows, out_cols,
    local_sem, send_sem, recv_sem,
):
    ny, nx = grid_of(n_sp)
    nz = n_tp // 2
    s, t = lax.axis_index("sp"), lax.axis_index("tp")
    y, x = s // nx, s % nx
    z, c = t // 2, t % 2
    features, positions = stream.shape
    channels = value_w.shape[1]
    f_cols = value_w.shape[2]
    c_cols = out_w.shape[2]
    width = channels * n_tp
    model = features * n_tp
    n_taps = taps.shape[0]
    reach = n_taps // 2
    groups = pieces_of(channels, LANES)
    group = channels // groups
    sends, recvs, sent = [0], [0], []

    def send_slot():
        sends[0] += 1
        return sends[0] - 1

    def recv_slot(count=1):
        recvs[0] += count
        return recvs[0] - count

    def remote(src, dst, sp, tp, send=None, recv=None):
        return pltpu.make_async_remote_copy(
            src_ref=src, dst_ref=dst,
            send_sem=send_sem.at[0 if send is None else send], recv_sem=recv_sem.at[0 if recv is None else recv],
            device_id={"sp": sp, "tp": tp}, device_id_type=MESH,
        )

    def start(copy, condition=None):
        if condition is None:
            copy.start()
        else:
            pl.when(condition)(copy.start)

    tag, banks = [None], {}

    def leave(ref, send, condition=None):
        sent.append((remote(ref, ref, s, t, send=send), condition, tag[0]))

    def finish_sends(name=None):
        chosen = [entry for entry in sent if name is None or entry[2] == name]
        sent[:] = [entry for entry in sent if name is not None and entry[2] != name]
        for entry in chosen:
            if entry[1] is None:
                entry[0].wait_send()
            else:
                pl.when(entry[1])(entry[0].wait_send)

    def banked(name, make):
        here, tag[0] = (sends[0], recvs[0]), name
        again = name in banks
        if again:
            assert not [entry for entry in sent if entry[2] == name]
            sends[0], recvs[0] = banks[name]
        banks.setdefault(name, here)
        made = make()
        if again:
            sends[0], recvs[0] = here
        tag[0] = None
        return made

    def slot_of(k, j):
        return lax.rem(y + ny - k, ny) * nx + lax.rem(x + nx - j, nx)

    def x_peer(j):
        return y * nx + lax.rem(x + j, nx)

    def y_peer(k):
        return lax.rem(y + k, ny) * nx + x

    local_count = [0]

    def local_copy(src, dst):
        i = local_count[0]
        local_count[0] += 1
        copy = pltpu.make_async_copy(src, dst, local_sem.at[i])
        copy.start()
        return copy

    class Gather:
        def __init__(self, src, dst, x_first, whole, send):
            self.copies, self.own_x, self.own_y, self.relays = {}, [], [], []
            for k in range(ny):
                for j in range(nx if whole else 1):
                    if k == 0 and j == 0:
                        continue
                    if x_first:
                        along_x = k == 0
                        origin = (0, 0) if along_x else (0, j)
                    else:
                        along_x = j > 0
                        origin = (k, 0) if along_x else (0, 0)
                    own = origin == (0, 0)
                    target = x_peer(j) if along_x else y_peer(k)
                    origin_slot = slot_of(*origin)
                    copy = remote(
                        src if own else dst(origin_slot), dst(origin_slot), target, t, send=send, recv=recv_slot()
                    )
                    self.copies[k, j] = copy
                    if not own:
                        self.relays.append((copy, origin))
                    elif along_x:
                        self.own_x.append(copy)
                    else:
                        self.own_y.append(copy)
            self.local = local_copy(src, dst(s))
            self.here, self.done = set(), set()

        def once(self, name):
            fresh = name not in self.done
            self.done.add(name)
            return fresh

        def send_x(self):
            if self.once("x"):
                for copy in self.own_x:
                    start(copy)

        def send_y(self):
            if self.once("y"):
                for copy in self.own_y:
                    start(copy)

        def relay(self):
            if self.once("relay"):
                for copy, origin in self.relays:
                    self.arrive(*origin)
                    start(copy)

        def flush(self):
            self.send_x()
            self.send_y()
            self.relay()

        def arrive(self, k, j):
            if (k, j) not in self.here:
                self.here.add((k, j))
                if k == 0 and j == 0:
                    self.local.wait()
                else:
                    self.copies[k, j].wait_recv()

    def gathers(w_ref, buf, l, orders, whole=True):
        rows = w_ref.shape[1] // len(orders)
        made, send = [], send_slot()
        leave(buf.at[l, pl.ds(0, (n_sp if whole else ny) - 1)], send)
        for i, x_first in enumerate(orders):
            part = pl.ds(i * rows, rows)
            made.append(Gather(w_ref.at[l, part], lambda q, part=part: buf.at[l, q, part], x_first, whole, send))
        return made

    class Spread:
        def __init__(self, pieces, at, whole, direct=False):
            def place(zz, cc, k):
                return at(jnp.clip(zz, 0, nz - 1) * 2 + cc, k)

            def full(zz, cc):
                return whole(jnp.clip(zz, 0, nz - 1) * 2 + cc)

            other = z * 2 + 1 - c
            self.pieces, self.place, self.direct = pieces, place, direct
            send, recv = send_slot(), recv_slot()
            self.across = [
                remote(place(z, c, k), place(z, c, k), s, other, send, recv) for k in range(pieces)
            ]
            self.landed = remote(full(z, 1 - c), full(z, 1 - c), s, other, recv=recv)
            leave(full(z, c), send)
            self.along, self.goes, self.hand, self.has, self.handed = {}, {}, {}, {}, {}
            for d in range(1, nz):
                for way in (1, -1):
                    has = (z - way * d >= 0) & (z - way * d < nz)
                    self.has[way, d] = has
                    send, hand_send, hand_recv = send_slot(), send_slot(), recv_slot()
                    if direct:
                        from_z, to_z = z, z + way * d
                        self.goes[way, d] = (to_z >= 0) & (to_z < nz)
                    else:
                        from_z, to_z = z - way * (d - 1), z + way
                        self.goes[way, d] = (from_z >= 0) & (from_z < nz) & (to_z >= 0) & (to_z < nz)
                    target = jnp.clip(to_z, 0, nz - 1) * 2 + c
                    for k in range(pieces):
                        held = place(from_z, c, k)
                        self.along[way, d, k] = remote(held, held, s, target, send, recv_slot())
                        seen = place(z - way * d, c, k)
                        self.hand[way, d, k] = remote(seen, seen, s, other, hand_send, hand_recv)
                    block = full(z - way * d, c)
                    self.handed[way, d] = remote(block, block, s, other, recv=hand_recv)
                    leave(block, send, self.goes[way, d])
                    leave(block, hand_send, has)

        def send(self, way, d, k):
            start(self.along[way, d, k], self.goes[way, d])

        def start_own(self, k):
            for d in range(1, nz) if self.direct else (1,):
                for way in (1, -1):
                    self.send(way, d, k)
            start(self.across[k])

        def step(self, d, k, extra=None):
            for way in (1, -1):
                pl.when(self.has[way, d])(self.along[way, d, k].wait_recv)
                if d + 1 < nz and not self.direct:
                    self.send(way, d + 1, k)
                start(self.hand[way, d, k], self.has[way, d])
                if extra is not None:
                    extra(way, d, k)

        def wait_across(self):
            self.landed.wait_recv()

        def wait_hand(self, way, d):
            self.handed[way, d].wait_recv()

    def ways_at(d):
        return (1, -1) if d else (1,)

    class Cross:
        def __init__(self, spread, land):
            self.spread, self.land = spread, land
            self.size = features // spread.pieces
            self.sends, self.base, self.hands = {}, {}, {}
            for d in range(nz):
                for way in ways_at(d):
                    ok, q, owner = self.facts(way, d)
                    block = self.rows(q, 0, spread.pieces)
                    self.sends[way, d] = send_slot()
                    leave(land.at[0, block, :], self.sends[way, d], ok & (owner != x))
                    for k in range(spread.pieces):
                        self.base[way, d, k] = recv_slot(nx - 1)
                    for j in range(1, nx):
                        send, recv = send_slot(), recv_slot()
                        place = land.at[j - 1, block, :]
                        mine = ok & (owner == x)
                        self.hands[way, d, j] = (send, recv, remote(place, place, s, t, recv=recv), mine)
                        leave(place, send, mine)

        def facts(self, way, d):
            zz = z - way * d
            ok = (zz >= 0) & (zz < nz)
            q = jnp.clip(zz, 0, nz - 1)
            return ok, q, lax.rem(q, nx)

        def rows(self, q, k, count=1):
            size = self.size
            row = (q // nx * 2 + c) * features + k * size
            return pl.ds(pl.multiple_of(row, size), size * count)

        def forward(self, way, d, k):
            ok, q, owner = self.facts(way, d)
            pick = jnp.clip(lax.rem(owner - x + nx, nx) - 1, 0, nx - 2)
            copy = remote(
                self.spread.place(q, c, k), self.land.at[pick, self.rows(q, k), :], y * nx + owner, t,
                self.sends[way, d], self.base[way, d, k] + pick,
            )
            start(copy, ok & (owner != x))

        def receive(self, way, d, k):
            _, q, _ = self.facts(way, d)
            for j in range(1, nx):
                send, recv, _, mine = self.hands[way, d, j]
                here = self.land.at[j - 1, self.rows(q, k), :]
                landed = remote(here, here, s, t, recv=self.base[way, d, k] + j - 1)
                hand = remote(here, here, s, z * 2 + 1 - c, send, recv)

                @pl.when(mine)
                def _():
                    landed.wait_recv()
                    hand.start()

        def receive_all(self, d):
            for k in range(self.spread.pieces):
                for way in ways_at(d):
                    self.receive(way, d, k)

        def finish(self):
            for _, _, handed, mine in self.hands.values():
                pl.when(mine)(handed.wait_recv)

    def exchange(src, buf):
        send, recv = send_slot(), recv_slot()
        others = buf.at[pl.ds(0, n_tp - 1)]
        for k in range(1, n_tp):
            start(remote(src, buf.at[t], s, lax.rem(t + k, n_tp), send, recv))
        leave(others, send)
        return [remote(others, others, s, t, recv=recv)]

    def arrived(copies):
        for copy in copies:
            copy.wait_recv()

    my_rows = pl.ds(pl.multiple_of(t * features, features), features)
    stream_pieces = pieces_of(features, 128)
    cuts = cuts_of(positions)

    def row_spread(buf):
        size = features // stream_pieces

        def at(block, k):
            return buf.at[pl.ds(pl.multiple_of(block * features + k * size, size), size), :]

        def whole(block):
            return buf.at[pl.ds(pl.multiple_of(block * features, features), features), :]

        return Spread(stream_pieces, at, whole)

    def position_spreads(inner, edge):
        return (
            Spread(
                len(cuts), lambda block, k: inner.at[block, pl.ds(cuts[k][0], cuts[k][1]), :],
                lambda block: inner.at[block, pl.ds(EDGE, positions - 2 * EDGE), :],
            ),
            Spread(1, lambda block, k: edge.at[block], lambda block: edge.at[block], direct=True),
        )

    stream_copy = local_copy(stream, h_all.at[0, my_rows, :])
    barrier = pltpu.get_barrier_semaphore()
    above, below = z + 1 < nz, z > 0
    near = [(x_peer(j), t, None) for j in range(1, nx)] + [(y_peer(k), t, None) for k in range(1, ny)]
    near += [(s, z * 2 + 1 - c, None), (s, (z + 1) * 2 + c, above), (s, (z - 1) * 2 + c, below)]
    for sp, tp, here in near:
        def greet(sp=sp, tp=tp):
            pl.semaphore_signal(barrier, inc=1, device_id={"sp": sp, "tp": tp}, device_id_type=MESH)

        if here is None:
            greet()
        else:
            pl.when(here)(greet)
    in_proj, out_proj = [], []
    out_parts = pieces_of(features, 128)
    for l in range(n_layers):
        in_proj.append(gathers(value_w, v_buf, l, [True], False) + gathers(gate_w, g_buf, l, [True], False))
        last = l + 1 == n_layers
        out_proj.append(gathers(out_w, o_buf, l, [last and i % 2 == 0 for i in range(out_parts)]))
    norm_rows[t] = norm_gain[...]
    out_rows[t] = out_gain[...]
    for l in range(n_layers):
        tap_rows[l, 0:n_taps, :] = taps[:, l, :].astype(F32)
    stream_copy.wait()
    @pl.when(above & below)
    def _():
        pl.semaphore_wait(barrier, nx + ny + 1)

    @pl.when(jnp.logical_not(above & below))
    def _():
        pl.semaphore_wait(barrier, nx + ny)

    spread = banked("rows", lambda: row_spread(h_all.at[0]))
    cross = banked("cross", lambda: Cross(spread, x_all.at[0]))
    for k in range(stream_pieces):
        spread.start_own(k)
        cross.forward(1, 0, k)
    early = max(1, out_parts // 2)
    for part in out_proj[0][:early]:
        part.send_x()
    for part in in_proj[0] + out_proj[0]:
        part.send_y()
    for l in range(1, n_layers):
        for part in in_proj[l]:
            part.send_y()

    def turn_gain(i):
        rows = out_rows[i].astype(F32)
        fill = jnp.zeros((8 - n_layers, features), F32)
        out_cols[i * features : (i + 1) * features, :] = jnp.concatenate([rows, fill], axis=0).T

    def across_lanes(a, b):
        return lax.dot_general(a, b, (((1,), (1,)), ((), ())), preferred_element_type=F32)

    turned = [0]
    steps = [(k, j) for k in range(ny) for j in range(nx)]
    right, left = lax.rem(s + 1, n_sp), lax.rem(s + n_sp - 1, n_sp)
    has_right, has_left = s < n_sp - 1, s > 0

    def rows_at(q, count):
        return pl.ds(pl.multiple_of(q * count, count), count)

    for l in range(n_layers):
        last = l + 1 == n_layers
        groups_of_rows = [pl.ds(m * group, group) for m in range(groups)]
        if l == 0:
            waiting = list(out_proj[0][early:])
            for d in range(1, nz):
                for k in range(stream_pieces):
                    spread.step(d, k, cross.forward)
                    for way in ways_at(d - 2) if d > 1 else ():
                        cross.receive(way, d - 2, k)
                    if waiting and ((d - 1) * stream_pieces + k) % 2 == 1:
                        waiting.pop(0).send_x()
            for part in waiting:
                part.send_x()
            spread.wait_across()
            for d in range(1, nz):
                for way in (1, -1):
                    @pl.when(spread.has[way, d])
                    def _():
                        spread.wait_hand(way, d)
            gain_copies = exchange(norm_gain, norm_rows) + exchange(out_gain, out_rows)
        if nz > 1:
            cross.receive_all(nz - 2)
        for half, (part, buf) in enumerate(zip(in_proj[l], (v_buf, g_buf))):
            total = None
            for k in range(ny):
                part.arrive(k, 0)
                slot = slot_of(k, 0)
                one = jnp.dot(buf[l, slot], h_all[l, rows_at(slot, f_cols), :], preferred_element_type=F32)
                total = one if total is None else total + one
            acc[half] = total
        cross.receive_all(nz - 1)
        cross.finish()
        if l > 0:
            for j in range(1, nx):
                factor_copies[j - 1].wait_recv()
                scale = peer_factor[l - 1, j - 1, 0:1, :]
                for k in range(ny):
                    here = pl.ds(k * f_cols, f_cols)
                    gain = out_cols[rows_at(k * nx + x, f_cols), l - 1 : l]
                    change = x_branch[l - 1, j - 1, here, :].astype(F32) * scale * gain
                    x_all[l, j - 1, here, :] = (x_all[l - 1, j - 1, here, :].astype(F32) + change).astype(BF16)
        part_copies = {}
        for m, rows in enumerate(groups_of_rows):
            for j in range(1, nx):
                for half, buf in enumerate((v_buf, g_buf)):
                    total = None
                    for k in range(ny):
                        block = rows_at(lax.rem(y + ny - k, ny), f_cols)
                        one = jnp.dot(
                            buf[l, slot_of(k, 0), rows, :], x_all[l, j - 1, block, :],
                            preferred_element_type=F32,
                        )
                        total = one if total is None else total + one
                    part_out[l, j - 1, half, rows, :] = total.astype(BF16)
                mine = part_out.at[l, j - 1, :, rows, :]
                send = send_slot()
                copy = remote(
                    mine, part_in.at[l, j - 1, :, rows, :], y * nx + lax.rem(x + nx - j, nx), t,
                    send, recv_slot(),
                )
                start(copy)
                leave(mine, send)
                part_copies[m, j] = copy

        edges = []
        for m, rows in enumerate(groups_of_rows):
            lanes = pl.ds(m * group, group)
            value, gate = acc[0, rows, :], acc[1, rows, :]
            for j in range(1, nx):
                part_copies[m, j].wait_recv()
                value = value + part_in[l, j - 1, 0, rows, :].astype(F32)
                gate = gate + part_in[l, j - 1, 1, rows, :].astype(F32)
            gated = (value * jax.nn.sigmoid(gate)).astype(BF16)
            wide[l, pl.ds(EDGE, positions), lanes] = gated.astype(F32).T
            pair = []
            for first, land, peer, here in (
                (positions, 0, right, has_right), (EDGE, EDGE + positions, left, has_left)
            ):
                mine, send = wide.at[l, pl.ds(first, EDGE), lanes], send_slot()
                copy = remote(mine, wide.at[l, pl.ds(land, EDGE), lanes], peer, t, send, recv_slot())
                start(copy, here)
                leave(mine, send, here)
                pair.append(copy)
            to_right, to_left = pair
            edges.append((to_right, to_left))

        for part in out_proj[l][:early] if l == 0 else out_proj[l]:
            part.flush()

        blank = jnp.zeros((EDGE, channels), F32)

        @pl.when(s == 0)
        def _():
            wide[l, 0:EDGE, :] = blank

        @pl.when(s == n_sp - 1)
        def _():
            wide[l, EDGE + positions : 2 * EDGE + positions, :] = blank

        def convolve(first, count, dst, land):
            while count:
                size = min(TILE, count)
                for m in range(groups):
                    lanes = pl.ds(m * group, group)
                    extent = size + 2 * EDGE
                    window = wide[l, pl.ds(first, extent), lanes]
                    total = None
                    for r in range(8):
                        moved = window if r == 0 else pltpu.roll(window, extent - r, 0)
                        for q in range(0, 2 * EDGE + 1, 8):
                            tap = q + r - (EDGE - reach)
                            if 0 <= tap < n_taps:
                                term = tap_rows[l, tap : tap + 1, lanes] * moved[q : q + size]
                                total = term if total is None else total + term
                    dst[l, t, pl.ds(land, size), lanes] = total.astype(BF16)
                first, land, count = first + size, land + size, count - size

        def total_up(phase, seen):
            square = seen.astype(F32) * seen.astype(F32)
            high = square.astype(BF16)
            low = (square - high.astype(F32)).astype(BF16)
            ones = jnp.ones((8, channels), BF16)
            sums[l, phase, t, 0:1, :] = across_lanes(ones, seen)[0:1]
            sums[l, phase, t, 1:2, :] = (across_lanes(ones, high) + across_lanes(ones, low))[0:1]
            return exchange(sums.at[l, phase, t], sums.at[l, phase])

        inner, edge = banked("conv", lambda: position_spreads(conv_all.at[l], conv_edge.at[l]))
        border = jnp.zeros((EDGE, channels), BF16)
        conv_all[l, t, 0:EDGE, :] = border
        conv_all[l, t, positions - EDGE : positions, :] = border
        for k, (first, count) in enumerate(cuts):
            convolve(first, count, conv_all, first)
            inner.start_own(k)
        sum_copies = [total_up(0, conv_all[l, t]), None]

        def finish_edges():
            for to_right, to_left in edges:
                pl.when(has_left)(to_right.wait_recv)
                pl.when(has_right)(to_left.wait_recv)
            convolve(0, EDGE, conv_edge, 0)
            convolve(positions - EDGE, EDGE, conv_edge, EDGE)
            edge.start_own(0)
            conv_all[l, t, 0:EDGE, :] = conv_edge[l, t, 0:EDGE, :]
            conv_all[l, t, positions - EDGE : positions, :] = conv_edge[l, t, EDGE : 2 * EDGE, :]
            sum_copies[1] = total_up(1, conv_all[l, t])

        def settle(phase):
            arrived(sum_copies[phase])
            totals = jnp.sum(sums[l, phase], axis=0)
            average = totals[0:1] / width
            variance = totals[1:2] / width - average * average
            for i, row in enumerate((average, lax.rsqrt(variance + 1e-05))):
                column = jnp.broadcast_to(row, (LANES, positions)).T
                if channels > LANES:
                    column = jnp.concatenate([column] * (channels // LANES), axis=1)
                stat_cols[i] = column[:, :channels]

        def activate(src, block, first, count, land):
            gain = norm_rows[block].astype(F32)[l : l + 1]
            place = pl.ds(land, count)
            seen = src[l, block, pl.ds(first, count), :].astype(F32)
            scaled = (seen - stat_cols[0, place, :]) * stat_cols[1, place, :] * gain
            active[block, place, :] = (scaled / (1.0 + jnp.exp(-scaled))).astype(BF16)

        def activate_inner(block):
            activate(conv_all, block, EDGE, positions - 2 * EDGE, EDGE)

        def drain(spread, ready, consume, hook, finish=None, extra=None):
            def take(d):
                for way in (1, -1):
                    @pl.when(spread.has[way, d])
                    def _():
                        consume((z - way * d) * 2 + c)
                        spread.wait_hand(way, d)
                        consume((z - way * d) * 2 + 1 - c)

            when = min(2, nz - 1)
            for d in range(1, nz):
                for k in range(spread.pieces):
                    spread.step(d, k, extra)
                    hook((d - 1) * spread.pieces + k)
                if d == when:
                    ready()
                    consume(t)
                    spread.wait_across()
                    consume(z * 2 + 1 - c)
                if d >= when and d > 1:
                    take(d - 1)
            if finish is not None:
                finish()
            take(nz - 1)

        def conv_hook(i):
            if i == min(1, len(cuts) - 1):
                finish_edges()
            if l == 0:
                if i == 2:
                    arrived(gain_copies)
                    finish_sends("rows")
                    finish_sends("cross")
                if i >= 2 and turned[0] < n_tp:
                    turn_gain(turned[0])
                    turned[0] += 1
                if i in (1, 3) and early + i // 2 < out_parts:
                    out_proj[l][early + i // 2].flush()
            if not last and i in (3, 5):
                for part in out_proj[l + 1][: i // 2]:
                    part.send_x()

        def catch_edges():
            for d in range(1, nz):
                edge.step(d, 0)

        drain(inner, lambda: settle(0), activate_inner, conv_hook, catch_edges)
        edge.wait_across()
        for d in range(1, nz):
            for way in (1, -1):
                @pl.when(edge.has[way, d])
                def _():
                    edge.wait_hand(way, d)
        settle(1)
        for block in range(n_tp):
            activate(conv_edge, block, 0, EDGE, 0)
            activate(conv_edge, block, EDGE, EDGE, positions - EDGE)
        while turned[0] < n_tp:
            turn_gain(turned[0])
            turned[0] += 1
        for part in out_proj[l]:
            part.flush()
        total = None
        for k, j in steps:
            slot = slot_of(k, j)
            for part in out_proj[l]:
                part.arrive(k, j)
            for i in range(c_cols // channels):
                one = across_lanes(
                    o_buf[l, slot, :, i * channels : (i + 1) * channels], active[slot * (c_cols // channels) + i]
                )
                total = one if total is None else total + one
        narrow_branch = total.astype(BF16)
        branch = narrow_branch.astype(F32)
        squares[l, t, 0:1, :] = jnp.sum(branch * branch, axis=0, keepdims=True)
        square_copies = exchange(squares.at[l, t], squares.at[l])

        def factor_of():
            arrived(square_copies)
            return lax.rsqrt(jnp.sum(squares[l], axis=0) / model + 1e-06)

        if last:
            factor = factor_of()
            gain = out_cols[my_rows, l : l + 1]
            fresh = h_all[l, my_rows, :].astype(F32) + branch * factor * gain
            result[...] = fresh.astype(BF16)
        else:
            branch_all[l, my_rows, :] = narrow_branch
            branch_spread = banked("rows", lambda: row_spread(branch_all.at[l]))
            cross = banked("cross", lambda: Cross(branch_spread, x_branch.at[l]))
            for k in range(stream_pieces):
                branch_spread.start_own(k)
                cross.forward(1, 0, k)
            for part in out_proj[l + 1]:
                part.send_y()

            factor, factor_copies = [None], []

            def scale_up():
                factor[0] = factor_of()
                own_factor[l, 0:1, :] = factor[0]
                for j in range(1, nx):
                    mine, send = own_factor.at[l], send_slot()
                    copy = remote(mine, peer_factor.at[l, j - 1], x_peer(j), t, send, recv_slot())
                    start(copy)
                    leave(mine, send)
                    factor_copies.append(copy)

            def renew(block):
                @pl.when((block == t) | (lax.rem(block // 2, nx) == x))
                def _():
                    rows = rows_at(block, features)
                    gain = out_cols[rows, l : l + 1]
                    change = branch_all[l, rows, :].astype(F32) * own_factor[l, 0:1, :] * gain
                    h_all[l + 1, rows, :] = (h_all[l, rows, :].astype(F32) + change).astype(BF16)

            def branch_hook(i):
                d, k = i // stream_pieces + 1, i % stream_pieces
                for way in ways_at(d - 2) if d > 1 else ():
                    cross.receive(way, d - 2, k)
                if i == 2:
                    finish_sends("conv")
                if i % 2 == 1 and 1 + i // 2 < out_parts:
                    out_proj[l + 1][1 + i // 2].send_x()

            drain(branch_spread, scale_up, renew, branch_hook, extra=cross.forward)

    finish_sends()
    assert sends[0] == send_sem.shape[0], sends
    assert recvs[0] == recv_sem.shape[0], recvs
    assert local_count[0] == local_sem.shape[0], local_count


def slots_of(ny, nx, nz, layers, features, channels, positions):
    n_sp, far = ny * nx, 2 * (nz - 1)
    pieces, cuts, groups = pieces_of(features, 128), len(cuts_of(positions)), pieces_of(channels, LANES)
    small = 2 + 3 * layers + groups * (nx - 1) * layers + 2 * groups * layers + (layers - 1) * (nx - 1)
    send = 3 * (1 + 2 * far) + (far + 1) * nx + 3 * layers + small
    recv = 3 + far * (pieces + 1 + cuts + 1 + 2) + (far + 1) * (pieces + 1) * (nx - 1) + small
    recv += layers * (2 * (ny - 1) + (n_sp - 1) * pieces)
    local = 1 + layers * (2 + pieces)
    return send, recv, local


def on_device(n_sp, n_tp, stream, value_weight, gate_weight, conv_taps, norm_gain, out_weight, out_gain):
    layers, channels, f_cols = value_weight.shape
    features, positions = stream.shape
    c_cols = out_weight.shape[2]
    ny, nx = grid_of(n_sp)
    send, recv, local = slots_of(ny, nx, n_tp // 2, layers, features, channels, positions)
    vmem = pl.BlockSpec(memory_space=pltpu.VMEM)
    hbm = pl.BlockSpec(memory_space=pl.ANY)
    return pl.pallas_call(
        functools.partial(kernel, n_sp, n_tp, layers),
        out_shape=jax.ShapeDtypeStruct(stream.shape, BF16),
        in_specs=[hbm, hbm, hbm, vmem, vmem, hbm, vmem],
        out_specs=vmem,
        scratch_shapes=[
            pltpu.VMEM((layers, n_tp * features, positions), BF16),
            pltpu.VMEM((layers, nx - 1, n_tp * features // nx, positions), BF16),
            pltpu.VMEM((max(layers - 1, 1), nx - 1, n_tp * features // nx, positions), BF16),
            pltpu.VMEM((layers, 1, positions), F32),
            pltpu.VMEM((layers, nx - 1, 1, positions), F32),
            pltpu.VMEM((layers, n_tp, positions, channels), BF16),
            pltpu.VMEM((layers, n_tp, 2 * EDGE, channels), BF16),
            pltpu.VMEM((max(layers - 1, 1), n_tp * features, positions), BF16),
            pltpu.VMEM((n_tp, positions, channels), BF16),
            pltpu.VMEM((layers, n_sp, channels, f_cols), BF16),
            pltpu.VMEM((layers, n_sp, channels, f_cols), BF16),
            pltpu.VMEM((layers, n_sp, features, c_cols), BF16),
            pltpu.VMEM((layers, nx - 1, 2, channels, positions), BF16),
            pltpu.VMEM((layers, nx - 1, 2, channels, positions), BF16),
            pltpu.VMEM((layers, positions + 2 * EDGE, channels), F32),
            pltpu.VMEM((2, positions, channels), F32),
            pltpu.VMEM((layers, 2 * EDGE, channels), F32),
            pltpu.VMEM((2, channels, positions), F32),
            pltpu.VMEM((layers, 2, n_tp, 2, positions), F32),
            pltpu.VMEM((layers, n_tp, 1, positions), F32),
            pltpu.VMEM((n_tp, layers, channels), BF16),
            pltpu.VMEM((n_tp, layers, features), BF16),
            pltpu.VMEM((n_tp * features, 8), F32),
            pltpu.SemaphoreType.DMA((local,)),
            pltpu.SemaphoreType.DMA((send,)),
            pltpu.SemaphoreType.DMA((recv,)),
        ],
        compiler_params=pltpu.CompilerParams(
            collective_id=0, has_side_effects=True, vmem_limit_bytes=60 * 1024 * 1024
        ),
    )(stream, value_weight, gate_weight, jnp.transpose(conv_taps, (2, 0, 1)), norm_gain, out_weight, out_gain)


def solution(mesh):
    return jax.shard_map(
        functools.partial(on_device, mesh.shape["sp"], mesh.shape["tp"]),
        mesh=mesh,
        in_specs=(
            P("tp", "sp"),
            P(None, "tp", "sp"),
            P(None, "tp", "sp"),
            P(None, "tp", None),
            P(None, "tp"),
            P(None, "tp", "sp"),
            P(None, "tp"),
        ),
        out_specs=P("tp", "sp"),
        check_vma=False,
    )
```
